128 devices in a mesh: kv: 16 (over z, y), tp: 8 (over x, core).
Axes of the slice: x: 4, y: 4, z: 4, core: 2. Of those that a mesh axis runs over, the one named last changes fastest.
Arguments:
- tokens: bfloat16 [128, 4096], P(None, 'kv'), may hold values from -8 to 8
- attn_gain: float32 [4096], P('kv'), may hold values from 0.1 to 1.9
- w_query: bfloat16 [4096, 2048], P('kv', 'tp'), may hold values from -0.09375 to 0.09375
- w_key: bfloat16 [4096, 2048], P('kv', 'tp'), may hold values from -0.09375 to 0.09375
- w_value: bfloat16 [4096, 4096], P('kv', 'tp'), may hold values from -0.09375 to 0.09375
- w_outgate: bfloat16 [4096, 4096], P('kv', 'tp'), may hold values from -0.09375 to 0.09375
- w_gates: bfloat16 [4096, 16], replicated, may hold values from -0.029907227 to 0.029907227
- forget_bias: float32 [8], replicated, may hold values from -1 to 3
- state_c: float32 [128, 8, 512, 256], P('kv', 'tp'), may hold values from -6 to 6
- state_n: float32 [128, 8, 256], P('kv', 'tp'), may hold values from -6 to 6
- state_m: float32 [128, 8], P('kv', 'tp'), may hold values from -2 to 0.5
- w_output: bfloat16 [4096, 4096], P('tp', 'kv'), may hold values from -0.09375 to 0.09375
- mlp_gain: float32 [4096], P('kv'), may hold values from 0.1 to 1.9
- w_gateff: bfloat16 [4096, 11008], P('kv', 'tp'), may hold values from -0.09375 to 0.09375
- w_upff: bfloat16 [4096, 11008], P('kv', 'tp'), may hold values from -0.09375 to 0.09375
- w_downff: bfloat16 [11008, 4096], P('tp', 'kv'), may hold values from -0.0546875 to 0.0546875
Outputs:
- mixed: bfloat16 [128, 4096], P(None, 'kv')
- new_c: float32 [128, 8, 512, 256], P('kv', 'tp')
- new_n: float32 [128, 8, 256], P('kv', 'tp')
- new_m: float32 [128, 8], P('kv', 'tp')
The draws below stay inside these ranges and needn't reach their ends.
All inputs are finite; a program needn't handle non-finite values.
Results may differ from the reference program's by a relative error of at most 0.0083.
Values may be sent and summed in bfloat16 or wider, within the bound.
A program may use at most 64 MiB of HBM per device.

```python
import math
import jax
import jax.numpy as jnp
from jax import lax

D = 4096
HEADS = 8
DQK = 256
DV = 512
FF = 11008
BATCH = 128


def draw_tokens(key, part):
    key_scale = jax.random.fold_in(key, 11)
    key_values = jax.random.fold_in(key, 12)
    groups = D // 16
    scales = jnp.exp(jax.random.uniform(key_scale, (groups,), jnp.float32, math.log(0.3), math.log(3.0)))
    scales = jnp.repeat(scales, 16)
    values = jax.random.normal(key_values, (BATCH, D), jnp.float32)
    return jnp.clip(values * scales[None, :], -8.0, 8.0).astype(jnp.bfloat16)


def level_of(rng, extent, shards, smallest, largest):
    def one(position, blocks):
        heights = jax.random.uniform(jax.random.fold_in(jax.random.fold_in(rng, 6), position), (blocks,), jnp.float32, smallest / len(shards), largest / len(shards))
        return jnp.repeat(jnp.exp(heights), extent[position] // blocks).reshape((-1,) + (1,) * (len(extent) - position - 1))

    loudness = one(*shards[0])
    for cut in shards[1:]:
        loudness = loudness * one(*cut)
    return loudness


def normal_values(stream_key, extent, deviation, limit, pieces=(), held_as=jnp.bfloat16):
    entries = jax.random.normal(stream_key, extent, jnp.float32) * deviation
    if len(pieces) > 0:
        entries = level_of(stream_key, extent, pieces, -0.22, 0.18) * entries
    return jnp.clip(entries, min=-limit, max=limit).astype(held_as)


def setup_inputs(seed: int = 0) -> dict:
    streams_of = jax.random.split(jax.random.key(seed), 17)
    return {
        "tokens": draw_tokens(jax.random.fold_in(streams_of[16], 71), 0),
        "attn_gain": jnp.clip(1.0 + 0.18 * jax.random.normal(streams_of[1], (D,), jnp.float32), 0.1, 1.9),
        "w_query": normal_values(streams_of[2], (D, HEADS * DQK), D ** -0.5, 0.09375, ((0, 16), (1, 8))),
        "w_key": normal_values(streams_of[3], (D, HEADS * DQK), D ** -0.5, 0.09375, ((0, 16), (1, 8))),
        "w_value": normal_values(streams_of[4], (D, HEADS * DV), D ** -0.5, 0.09375, ((0, 16), (1, 8))),
        "w_outgate": normal_values(streams_of[5], (D, HEADS * DV), D ** -0.5, 0.09375, ((0, 16), (1, 8))),
        "w_gates": normal_values(streams_of[6], (D, 2 * HEADS), 0.0047, 0.029907227),
        "forget_bias": jnp.clip(jax.random.uniform(streams_of[7], (HEADS,), jnp.float32, -1.0, 3.0), -1.0, 3.0),
        "state_c": normal_values(streams_of[8], (BATCH, HEADS, DV, DQK), 1.0, 6.0, ((0, 16), (1, 8)), jnp.float32),
        "state_n": normal_values(streams_of[9], (BATCH, HEADS, DQK), 1.0, 6.0, ((0, 16), (1, 8)), jnp.float32),
        "state_m": jnp.clip(-2.0 + 2.5 * jax.random.uniform(streams_of[10], (BATCH, HEADS), jnp.float32) ** level_of(streams_of[10], (BATCH, HEADS), ((0, 16), (1, 8)), -0.2, 0.2), -2.0, 0.5),
        "w_output": normal_values(streams_of[11], (HEADS * DV, D), (HEADS * DV) ** -0.5, 0.09375, ((0, 8), (1, 16))),
        "mlp_gain": jnp.clip(1.0 + 0.18 * jax.random.normal(streams_of[12], (D,), jnp.float32), 0.1, 1.9),
        "w_gateff": normal_values(streams_of[13], (D, FF), D ** -0.5, 0.09375, ((0, 16), (1, 8))),
        "w_upff": normal_values(streams_of[14], (D, FF), D ** -0.5, 0.09375, ((0, 16), (1, 8))),
        "w_downff": normal_values(streams_of[15], (FF, D), FF ** -0.5, 0.0546875, ((0, 8), (1, 16))),
    }


norm_floor = 1e-05

def inverse_rms(values):
    return lax.rsqrt(lax.optimization_barrier(jnp.mean(values * values, axis=-1)) + norm_floor)

def reference(tokens, attn_gain, w_query, w_key, w_value, w_outgate, w_gates, forget_bias, state_c, state_n, state_m, w_output, mlp_gain, w_gateff, w_upff, w_downff):
    batch = tokens.shape[0]
    tok_float = tokens.astype(jnp.float32)
    scale_one = inverse_rms(tok_float)[:, None]
    normed_one = (tok_float * attn_gain).astype(jnp.bfloat16)

    def project(weight):
        return jnp.dot(normed_one, weight, preferred_element_type=jnp.float32) * scale_one
    query = (project(w_query) * DQK ** (-0.5)).reshape(batch, HEADS, DQK)
    key_vec = project(w_key).reshape(batch, HEADS, DQK)
    value = project(w_value).reshape(batch, HEADS, DV)
    out_pre = project(w_outgate).reshape(batch, HEADS, DV)
    gate_pre = project(w_gates)
    log_input = gate_pre[:, :HEADS]
    log_forget = jax.nn.log_sigmoid(gate_pre[:, HEADS:] + forget_bias)
    carried = log_forget + state_m
    new_m = jnp.maximum(carried, log_input)
    keep = jnp.exp(carried - new_m)
    admit = jnp.exp(log_input - new_m)
    new_c = keep[:, :, None, None] * state_c + admit[:, :, None, None] * value[:, :, :, None] * key_vec[:, :, None, :]
    new_n = keep[:, :, None] * state_n + admit[:, :, None] * key_vec
    numer = jnp.einsum('bhvd,bhd->bhv', new_c, query, precision=lax.Precision.HIGHEST)
    denom = jnp.maximum(jnp.abs(lax.optimization_barrier(jnp.sum(new_n * query, axis=-1))), jnp.exp(-new_m))
    head_out = (jax.nn.sigmoid(out_pre) * numer / denom[:, :, None]).reshape(batch, HEADS * DV).astype(jnp.bfloat16)
    attn_mix = jnp.dot(head_out, w_output, preferred_element_type=jnp.float32)
    middle = (tok_float + attn_mix).astype(jnp.bfloat16)
    mid_float = middle.astype(jnp.float32)
    scale_two = inverse_rms(mid_float)[:, None]
    normed_two = (mid_float * mlp_gain).astype(jnp.bfloat16)
    gate_ff = jnp.dot(normed_two, w_gateff, preferred_element_type=jnp.float32) * scale_two
    up_ff = jnp.dot(normed_two, w_upff, preferred_element_type=jnp.float32) * scale_two
    hidden_ff = (jax.nn.silu(gate_ff) * up_ff).astype(jnp.bfloat16)
    mixed = (mid_float + jnp.dot(hidden_ff, w_downff, preferred_element_type=jnp.float32)).astype(jnp.bfloat16)
    return (mixed, new_c, new_n, new_m)
```

```python
import functools

import jax
import jax.numpy as jnp
from jax import lax
from jax.experimental import pallas as pl
from jax.experimental.pallas import tpu as pltpu
from jax.sharding import PartitionSpec as P

MESH = pl.DeviceIdType.MESH
norm_floor = 1e-05
f32 = jnp.float32
bf16 = jnp.bfloat16
LANES = 128


def up_to_lanes(length):
    return (length + LANES - 1) // LANES * LANES


def dot(a, b):
    return jnp.dot(a, b, preferred_element_type=f32)


def dot_rows(a, b):
    return lax.dot_general(a, b, (((1,), (1,)), ((), ())), preferred_element_type=f32)


def lane_ids(rows):
    return lax.broadcasted_iota(jnp.int32, (rows, LANES), 1)


def layer(
    kv_n,
    tp_n,
    tokens,
    attn_gain,
    w_query,
    w_key,
    w_value,
    w_outgate,
    w_gates,
    forget_bias,
    state_c,
    state_n,
    state_m,
    w_output,
    mlp_gain,
    w_gateff,
    w_upff,
    w_downff,
    mixed,
    new_c,
    new_n,
    new_m,
    tok_v,
    gain_one_v,
    w_proj_v,
    w_gates_v,
    bias_v,
    c_v,
    n_v,
    m_v,
    w_out_v,
    gain_two_v,
    w_gateff_v,
    w_upff_v,
    w_down_v,
    c_short,
    c_new,
    n_new,
    m_new,
    proj_send,
    proj_recv,
    head_all,
    attn_send,
    attn_recv,
    mid_all,
    ff_send,
    ff_recv,
    hidden_all,
    down_send,
    down_recv,
    mixed_all,
    in_sem,
    out_sem,
    kv_send_sem,
    kv_recv_sem,
    tp_send_sem,
    tp_recv_sem,
):
    kv = lax.axis_index("kv")
    tp = lax.axis_index("tp")
    batch, width = tok_v.shape
    rows = batch // kv_n
    tp_rows = batch // tp_n
    width_all = width * kv_n
    heads_all = bias_v.shape[1]
    value_size, query_size = c_v.shape[1:]
    proj_width = w_proj_v.shape[1]
    ff = w_gateff_v.shape[0]
    ff_pad = up_to_lanes(ff)

    loads = []

    def load(source, target):
        copy = pltpu.make_async_copy(source, target, in_sem.at[len(loads)])
        copy.start()
        loads.append(copy)
        return copy

    first = [load(tokens, tok_v), load(attn_gain, gain_one_v)]
    at = 0
    for weight in (w_query, w_key, w_value, w_outgate):
        columns = weight.shape[1]
        first.append(load(weight, w_proj_v.at[:, pl.ds(at, columns)]))
        at += columns
    first.append(load(w_gates.at[:, pl.ds(pl.multiple_of(kv * width, width), width)], w_gates_v))
    load_c = load(state_c.at[:, 0], c_v)
    load_cell = [load(state_n, n_v), load(state_m, m_v), load(forget_bias, bias_v)]
    load_out = load(w_output, w_out_v)
    load_ff = [load(mlp_gain, gain_two_v), load(w_gateff, w_gateff_v), load(w_upff, w_upff_v)]
    load_down = load(w_downff, w_down_v)

    barrier = pltpu.get_barrier_semaphore()

    def greet_kv(step, carry):
        pl.semaphore_signal(
            barrier, inc=1, device_id={"kv": lax.rem(kv + step, kv_n)}, device_id_type=MESH
        )
        return carry

    def greet_tp(step, carry):
        pl.semaphore_signal(
            barrier, inc=1, device_id={"tp": lax.rem(tp + step, tp_n)}, device_id_type=MESH
        )
        return carry

    lax.fori_loop(1, kv_n, greet_kv, 0)
    lax.fori_loop(1, tp_n, greet_tp, 0)

    def exchange(axis, phase, source_of, target):
        me, count = (kv, kv_n) if axis == "kv" else (tp, tp_n)
        sends, recvs = (kv_send_sem, kv_recv_sem) if axis == "kv" else (tp_send_sem, tp_recv_sem)

        def copy_to(peer):
            return pltpu.make_async_remote_copy(
                src_ref=source_of(peer),
                dst_ref=target.at[me],
                send_sem=sends.at[phase, peer],
                recv_sem=recvs.at[phase, me],
                device_id={axis: peer},
                device_id_type=MESH,
            )

        def copy_from(peer):
            return pltpu.make_async_remote_copy(
                src_ref=source_of(peer),
                dst_ref=target.at[peer],
                send_sem=sends.at[phase, peer],
                recv_sem=recvs.at[phase, peer],
                device_id={axis: peer},
                device_id_type=MESH,
            )

        def start(step, carry):
            copy_to(lax.rem(me + step, count)).start()
            return carry

        lax.fori_loop(1, count, start, 0)

        def arrived(step):
            peer = lax.rem(me + step, count)
            copy_from(peer).wait_recv()
            return peer

        def all_arrived():
            def wait(step, carry):
                arrived(step)
                return carry

            lax.fori_loop(1, count, wait, 0)

        def sent():
            def wait(step, carry):
                copy_to(lax.rem(me + step, count)).wait_send()
                return carry

            lax.fori_loop(1, count, wait, 0)

        def total(own):
            def add(step, carry):
                return carry + target[arrived(step)].astype(f32)

            return lax.fori_loop(1, count, add, own)

        return all_arrived, total, sent

    for copy in first:
        copy.wait()
    tok_float = tok_v[...].astype(f32)
    squares_one = jnp.sum(tok_float * tok_float, axis=1, keepdims=True)
    normed_one = (tok_float * gain_one_v[...]).astype(bf16)
    lanes = lane_ids(batch)
    gate_row = lax.broadcasted_iota(jnp.int32, (LANES, 2 * heads_all), 1)
    gate_lane = lax.broadcasted_iota(jnp.int32, (LANES, 2 * heads_all), 0)
    wanted = jnp.where(
        (gate_lane == 0) | (gate_lane == 3),
        tp,
        jnp.where((gate_lane == 1) | (gate_lane == 4), heads_all + tp, -1),
    )
    pick = jnp.where(gate_row == wanted, 1.0, 0.0).astype(bf16)
    gate_weight = dot(pick, w_gates_v[...]).astype(bf16)
    extra = dot_rows(normed_one, gate_weight)
    extra = jnp.where((lanes == 2) | (lanes == 5), squares_one, extra)
    extra_short = extra.astype(bf16).astype(f32)
    extra = jnp.where(lanes < 3, extra_short, extra - extra_short)
    proj_send[:, :, pl.ds(proj_width, LANES)] = extra.reshape(kv_n, rows, LANES).astype(bf16)
    step = 512
    for at in range(0, proj_width, step):
        part = dot(normed_one, w_proj_v[:, pl.ds(at, step)])
        proj_send[:, :, pl.ds(at, step)] = part.reshape(kv_n, rows, step).astype(bf16)

    pl.semaphore_wait(barrier, kv_n + tp_n - 2)
    _, proj_total, proj_sent = exchange("kv", 0, lambda peer: proj_send.at[peer], proj_recv)

    load_c.wait()
    for one in range(rows):
        c_short[one] = c_v[one].astype(bf16)
    for copy in load_cell:
        copy.wait()

    proj_rows = proj_total(proj_send[kv].astype(f32))
    extra = proj_rows[:, proj_width:]
    lanes = lane_ids(rows)

    def picked(lane):
        chosen = (lanes == lane) | (lanes == lane + 3)
        return jnp.sum(jnp.where(chosen, extra, 0.0), axis=1, keepdims=True)

    scale_one = lax.rsqrt(picked(2) / width_all + norm_floor)
    proj_rows = proj_rows[:, :proj_width] * scale_one
    query = proj_rows[:, :query_size] * query_size ** (-0.5)
    key_vec = proj_rows[:, query_size : 2 * query_size]
    value = proj_rows[:, 2 * query_size : 2 * query_size + value_size]
    out_pre = proj_rows[:, 2 * query_size + value_size :]
    head_lane = lax.broadcasted_iota(jnp.int32, (1, heads_all), 1)
    bias = jnp.sum(jnp.where(head_lane == tp, bias_v[...], 0.0), axis=1, keepdims=True)
    log_input = picked(0) * scale_one
    forget_pre = picked(1) * scale_one + bias
    log_forget = -(jnp.maximum(-forget_pre, 0.0) + jnp.log1p(jnp.exp(-jnp.abs(forget_pre))))
    row_at = lax.broadcasted_iota(jnp.int32, (rows, rows), 0)
    same = row_at == lax.broadcasted_iota(jnp.int32, (rows, rows), 1)
    m_column = jnp.sum(jnp.where(same, m_v[...], 0.0), axis=1, keepdims=True)
    carried = log_forget + m_column
    m_next = jnp.maximum(carried, log_input)
    keep = jnp.exp(carried - m_next)
    admit = jnp.exp(log_input - m_next)
    n_next = keep * n_v[:, 0, :] + admit * key_vec
    denom = jnp.maximum(
        jnp.abs(jnp.sum(n_next * query, axis=1, keepdims=True)), jnp.exp(-m_next)
    )
    key_query = jnp.sum(key_vec * query, axis=1, keepdims=True)
    query_short = query.astype(bf16)
    query_rest = (query - query_short.astype(f32)).astype(bf16)
    row_ids = lax.broadcasted_iota(jnp.int32, (rows, value_size), 0)
    read = jnp.zeros((rows, value_size), f32)
    query_both = jnp.concatenate([query_short.astype(f32), query_rest.astype(f32)], axis=0).astype(bf16)
    for one in range(rows):
        product = dot_rows(query_both, c_short[one])
        read = jnp.where(row_ids == one, product[:rows] + product[rows:], read)
    admitted = admit * value
    numer = keep * read + admitted * key_query
    head_all[kv] = (jax.nn.sigmoid(out_pre) * numer / denom).astype(bf16)
    head_arrived, _, head_sent = exchange("kv", 1, lambda peer: head_all.at[kv], head_all)

    n_new[:, 0, :] = n_next
    m_new[...] = jnp.sum(jnp.where(same, m_next, 0.0), axis=0, keepdims=True)
    stores = [
        pltpu.make_async_copy(n_new, new_n, out_sem.at[0]),
        pltpu.make_async_copy(m_new, new_m, out_sem.at[1]),
    ]
    for copy in stores:
        copy.start()
    admitted_column = admitted.T
    for one in range(rows):
        c_new[one] = (
            keep[one : one + 1, :] * c_v[one]
            + admitted_column[:, one : one + 1] * key_vec[one : one + 1, :]
        )
        copy = pltpu.make_async_copy(c_new.at[one], new_c.at[one, 0], out_sem.at[2 + one])
        copy.start()
        stores.append(copy)

    load_out.wait()
    head_arrived()
    heads = head_all[...].astype(f32).reshape(batch, value_size).astype(bf16)
    attn_part = dot(heads, w_out_v[...])
    attn_send[...] = attn_part.reshape(tp_n, tp_rows, width).astype(bf16)
    _, attn_total, attn_sent = exchange("tp", 0, lambda peer: attn_send.at[peer], attn_recv)
    own_rows = pl.ds(pl.multiple_of(tp * tp_rows, tp_rows), tp_rows)
    attn_mix = attn_total(attn_send[tp].astype(f32))
    mid_all[tp] = (tok_v[own_rows, :].astype(f32) + attn_mix).astype(bf16)
    mid_arrived, _, mid_sent = exchange("tp", 1, lambda peer: mid_all.at[tp], mid_all)
    for copy in load_ff:
        copy.wait()
    mid_arrived()

    mid_float = mid_all[...].astype(f32).reshape(batch, width)
    squares_two = jnp.sum(mid_float * mid_float, axis=1, keepdims=True)
    normed_two = (mid_float * gain_two_v[...]).astype(bf16)
    lanes = lane_ids(batch)
    squares_short = squares_two.astype(bf16).astype(f32)
    extra = jnp.where(
        lanes == 0, squares_short, jnp.where(lanes == 1, squares_two - squares_short, 0.0)
    )
    ff_send[:, :, pl.ds(2 * ff_pad, LANES)] = extra.reshape(kv_n, rows, LANES).astype(bf16)
    for base, weight in ((0, w_gateff_v), (ff_pad, w_upff_v)):
        for at in range(0, ff, step):
            columns = min(step, ff - at)
            part = dot_rows(normed_two, weight[pl.ds(at, columns), :])
            ff_send[:, :, pl.ds(base + at, columns)] = part.reshape(kv_n, rows, columns).astype(bf16)
    _, ff_total, ff_sent = exchange("kv", 2, lambda peer: ff_send.at[peer], ff_recv)
    ff_rows = ff_total(ff_send[kv].astype(f32))
    rows_two = jnp.sum(ff_rows[:, 2 * ff_pad :], axis=1, keepdims=True)
    scale_two = lax.rsqrt(rows_two / width_all + norm_floor)
    gate_ff = ff_rows[:, :ff] * scale_two
    up_ff = ff_rows[:, ff_pad : ff_pad + ff] * scale_two
    hidden_all[kv] = (gate_ff / (1.0 + jnp.exp(-gate_ff)) * up_ff).astype(bf16)
    hidden_arrived, _, hidden_sent = exchange("kv", 3, lambda peer: hidden_all.at[kv], hidden_all)

    load_down.wait()
    hidden_arrived()
    hidden = hidden_all[...].astype(f32).reshape(batch, ff).astype(bf16)
    down_part = dot(hidden, w_down_v[...])
    down_send[...] = down_part.reshape(tp_n, tp_rows, width).astype(bf16)
    _, down_total, down_sent = exchange("tp", 2, lambda peer: down_send.at[peer], down_recv)
    down_sum = down_total(down_send[tp].astype(f32))
    mixed_all[tp] = (mid_all[tp].astype(f32) + down_sum).astype(bf16)
    mixed_arrived, _, mixed_sent = exchange("tp", 3, lambda peer: mixed_all.at[tp], mixed_all)
    for sent in (proj_sent, head_sent, attn_sent, mid_sent, ff_sent, hidden_sent, down_sent):
        sent()
    for copy in stores:
        copy.wait()
    mixed_arrived()
    for slot in range(tp_n):
        pltpu.make_async_copy(
            mixed_all.at[slot], mixed.at[pl.ds(slot * tp_rows, tp_rows)], in_sem.at[slot]
        ).start()
    for slot in range(tp_n):
        pltpu.make_async_copy(
            mixed_all.at[slot], mixed.at[pl.ds(slot * tp_rows, tp_rows)], in_sem.at[slot]
        ).wait()
    mixed_sent()


def solution(mesh):
    kv_n, tp_n = mesh.shape["kv"], mesh.shape["tp"]

    def per_device(*args):
        args = list(args)
        for place in (1, 7, 12):
            args[place] = args[place].reshape(1, -1)
        for place in (6, 10, 13, 14):
            args[place] = args[place].T
        tokens, w_query, w_value, state_c, w_gateff = (args[i] for i in (0, 2, 4, 8, 13))
        batch, width = tokens.shape
        rows, tp_rows = batch // kv_n, batch // tp_n
        value_size, query_size = state_c.shape[2:]
        ff = w_gateff.shape[0]
        ff_pad = up_to_lanes(ff)
        proj_width = 2 * query_size + 2 * value_size
        heads_all = args[7].shape[1]
        V = pltpu.VMEM
        scratch = [
            V((batch, width), bf16),
            V((1, width), f32),
            V((width, proj_width), bf16),
            V((2 * heads_all, width), bf16),
            V((1, heads_all), f32),
            V((rows, value_size, query_size), f32),
            V((rows, 1, query_size), f32),
            V((1, rows), f32),
            V((value_size, width), bf16),
            V((1, width), f32),
            V((ff, width), bf16),
            V((ff, width), bf16),
            V((ff, width), bf16),
            V((rows, value_size, query_size), bf16),
            V((rows, value_size, query_size), f32),
            V((rows, 1, query_size), f32),
            V((1, rows), f32),
            V((kv_n, rows, proj_width + LANES), bf16),
            V((kv_n, rows, proj_width + LANES), bf16),
            V((kv_n, rows, value_size), bf16),
            V((tp_n, tp_rows, width), bf16),
            V((tp_n, tp_rows, width), bf16),
            V((tp_n, tp_rows, width), bf16),
            V((kv_n, rows, 2 * ff_pad + LANES), bf16),
            V((kv_n, rows, 2 * ff_pad + LANES), bf16),
            V((kv_n, rows, ff), bf16),
            V((tp_n, tp_rows, width), bf16),
            V((tp_n, tp_rows, width), bf16),
            V((tp_n, tp_rows, width), bf16),
            pltpu.SemaphoreType.DMA((16,)),
            pltpu.SemaphoreType.DMA((2 + rows,)),
            pltpu.SemaphoreType.DMA((4, kv_n)),
            pltpu.SemaphoreType.DMA((4, kv_n)),
            pltpu.SemaphoreType.DMA((4, tp_n)),
            pltpu.SemaphoreType.DMA((4, tp_n)),
        ]
        anywhere = pl.BlockSpec(memory_space=pl.ANY)
        outs = pl.pallas_call(
            functools.partial(layer, kv_n, tp_n),
            out_shape=(
                jax.ShapeDtypeStruct((batch, width), bf16),
                jax.ShapeDtypeStruct(state_c.shape, f32),
                jax.ShapeDtypeStruct(args[9].shape, f32),
                jax.ShapeDtypeStruct(args[10].shape, f32),
            ),
            in_specs=[anywhere] * len(args),
            out_specs=(anywhere,) * 4,
            scratch_shapes=scratch,
            compiler_params=pltpu.CompilerParams(
                collective_id=0, has_side_effects=True, vmem_limit_bytes=60 * 1024 * 1024
            ),
        )(*args)
        return (*outs[:3], outs[3].T)

    placed = (
        P(None, "kv"),
        P("kv"),
        P("kv", "tp"),
        P("kv", "tp"),
        P("kv", "tp"),
        P("kv", "tp"),
        P(),
        P(),
        P("kv", "tp", None, None),
        P("kv", "tp", None),
        P("kv", "tp"),
        P("tp", "kv"),
        P("kv"),
        P("kv", "tp"),
        P("kv", "tp"),
        P("tp", "kv"),
    )
    return jax.shard_map(
        per_device,
        mesh=mesh,
        in_specs=placed,
        out_specs=(P(None, "kv"), P("kv", "tp", None, None), P("kv", "tp", None), P("kv", "tp")),
        check_vma=False,
    )
```

```python
import functools

import jax
import jax.numpy as jnp
from jax import lax
from jax.experimental import pallas as pl
from jax.experimental.pallas import tpu as pltpu
from jax.sharding import PartitionSpec as P

MESH = pl.DeviceIdType.MESH
norm_floor = 1e-05
f32 = jnp.float32
bf16 = jnp.bfloat16
LANES = 128


def up_to_lanes(length):
    return (length + LANES - 1) // LANES * LANES


def dot(a, b):
    return jnp.dot(a, b, preferred_element_type=f32)


def dot_rows(a, b):
    return lax.dot_general(a, b, (((1,), (1,)), ((), ())), preferred_element_type=f32)


def lane_ids(rows):
    return lax.broadcasted_iota(jnp.int32, (rows, LANES), 1)


def layer(
    kv_n,
    tp_n,
    tokens,
    attn_gain,
    w_query,
    w_key,
    w_value,
    w_outgate,
    w_gates,
    forget_bias,
    state_c,
    state_n,
    state_m,
    w_output,
    mlp_gain,
    w_gateff,
    w_upff,
    w_downff,
    mixed,
    new_c,
    new_n,
    new_m,
    tok_v,
    gain_one_v,
    w_proj_v,
    w_gates_v,
    bias_v,
    c_v,
    n_v,
    m_v,
    w_out_v,
    gain_two_v,
    w_gateff_v,
    w_upff_v,
    w_down_v,
    c_short,
    proj_send,
    proj_recv,
    head_all,
    attn_send,
    attn_recv,
    mid_all,
    ff_send,
    ff_recv,
    hidden_all,
    down_send,
    down_recv,
    in_sem,
    kv_send_sem,
    kv_recv_sem,
    tp_send_sem,
    tp_recv_sem,
):
    kv = lax.axis_index("kv")
    tp = lax.axis_index("tp")
    batch, width = tok_v.shape
    rows = batch // kv_n
    tp_rows = batch // tp_n
    width_all = width * kv_n
    heads_all = bias_v.shape[1]
    value_size, query_size = c_v.shape[1:]
    proj_width = w_proj_v.shape[1]
    ff = w_gateff_v.shape[0]
    ff_pad = up_to_lanes(ff)

    near = {0: 0, 1: 1, 2: 2, 3: 1}
    side = 4

    def peer_at(axis, offset):
        first, second = offset
        if axis == "kv":
            return lax.rem(kv // side + first, side) * side + lax.rem(kv % side + second, side)
        return lax.rem(tp // 2 + first, side) * 2 + lax.rem(tp % 2 + second, 2)

    kv_order = [(a, b) for a in range(side) for b in range(side) if a or b]
    kv_order.sort(key=lambda offset: -near[offset[0]] - near[offset[1]])
    tp_order = [(a, b) for a in range(side) for b in range(2) if a or b]
    tp_order.sort(key=lambda offset: -near[offset[0]])

    barrier = pltpu.get_barrier_semaphore()

    def greet_kv(step, carry):
        pl.semaphore_signal(
            barrier, inc=1, device_id={"kv": lax.rem(kv + step, kv_n)}, device_id_type=MESH
        )
        return carry

    def greet_tp(step, carry):
        pl.semaphore_signal(
            barrier, inc=1, device_id={"tp": lax.rem(tp + step, tp_n)}, device_id_type=MESH
        )
        return carry

    lax.fori_loop(1, kv_n, greet_kv, 0)
    lax.fori_loop(1, tp_n, greet_tp, 0)

    loads = []

    def load(source, target):
        copy = pltpu.make_async_copy(source, target, in_sem.at[len(loads)])
        copy.start()
        loads.append(copy)
        return copy

    first = [load(tokens, tok_v), load(attn_gain, gain_one_v)]
    at = 0
    for weight in (w_query, w_key, w_value, w_outgate):
        columns = weight.shape[1]
        first.append(load(weight, w_proj_v.at[:, pl.ds(at, columns)]))
        at += columns
    first.append(load(w_gates.at[:, pl.ds(pl.multiple_of(kv * width, width), width)], w_gates_v))
    load_c = load(state_c.at[:, 0], c_v)
    load_cell = [load(state_n, n_v), load(state_m, m_v), load(forget_bias, bias_v)]
    load_out = load(w_output, w_out_v)
    load_ff = [load(mlp_gain, gain_two_v), load(w_gateff, w_gateff_v), load(w_upff, w_upff_v)]
    load_down = load(w_downff, w_down_v)

    def exchange(axis, phase, source_of, target):
        me, count = (kv, kv_n) if axis == "kv" else (tp, tp_n)
        sends, recvs = (kv_send_sem, kv_recv_sem) if axis == "kv" else (tp_send_sem, tp_recv_sem)

        def copy_to(peer):
            return pltpu.make_async_remote_copy(
                src_ref=source_of(peer),
                dst_ref=target.at[me],
                send_sem=sends.at[phase, peer],
                recv_sem=recvs.at[phase, me],
                device_id={axis: peer},
                device_id_type=MESH,
            )

        def copy_from(peer):
            return pltpu.make_async_remote_copy(
                src_ref=source_of(peer),
                dst_ref=target.at[peer],
                send_sem=sends.at[phase, peer],
                recv_sem=recvs.at[phase, peer],
                device_id={axis: peer},
                device_id_type=MESH,
            )

        order = kv_order if axis == "kv" else tp_order
        for offset in order:
            copy_to(peer_at(axis, offset)).start()

        def arrived(step):
            peer = lax.rem(me + step, count)
            copy_from(peer).wait_recv()
            return peer

        def all_arrived():
            def wait(step, carry):
                arrived(step)
                return carry

            lax.fori_loop(1, count, wait, 0)

        def sent():
            def wait(step, carry):
                copy_to(lax.rem(me + step, count)).wait_send()
                return carry

            lax.fori_loop(1, count, wait, 0)

        def total(own):
            def add(step, carry):
                return carry + target[arrived(step)].astype(f32)

            return lax.fori_loop(1, count, add, own)

        return all_arrived, total, sent

    for copy in first:
        copy.wait()
    tok_float = tok_v[...].astype(f32)
    squares_one = jnp.sum(tok_float * tok_float, axis=1, keepdims=True)
    normed_one = (tok_float * gain_one_v[...]).astype(bf16)
    lanes = lane_ids(batch)
    gate_row = lax.broadcasted_iota(jnp.int32, (LANES, 2 * heads_all), 1)
    gate_lane = lax.broadcasted_iota(jnp.int32, (LANES, 2 * heads_all), 0)
    wanted = jnp.where(
        (gate_lane == 0) | (gate_lane == 3),
        tp,
        jnp.where((gate_lane == 1) | (gate_lane == 4), heads_all + tp, -1),
    )
    pick = jnp.where(gate_row == wanted, 1.0, 0.0).astype(bf16)
    gate_weight = dot(pick, w_gates_v[...]).astype(bf16)
    extra = dot_rows(normed_one, gate_weight)
    extra = jnp.where((lanes == 2) | (lanes == 5), squares_one, extra)
    extra_short = extra.astype(bf16).astype(f32)
    extra = jnp.where(lanes < 3, extra_short, extra - extra_short)
    proj_send[:, :, pl.ds(proj_width, LANES)] = extra.reshape(kv_n, rows, LANES).astype(bf16)
    step = 512
    for at in range(0, proj_width, step):
        part = dot(normed_one, w_proj_v[:, pl.ds(at, step)])
        proj_send[:, :, pl.ds(at, step)] = part.reshape(kv_n, rows, step).astype(bf16)

    pl.semaphore_wait(barrier, kv_n + tp_n - 2)
    _, proj_total, proj_sent = exchange("kv", 0, lambda peer: proj_send.at[peer], proj_recv)

    load_c.wait()
    for one in range(rows):
        c_short[one] = c_v[one].astype(bf16)
    for copy in load_cell:
        copy.wait()

    proj_rows = proj_total(proj_send[kv].astype(f32))
    extra = proj_rows[:, proj_width:]
    lanes = lane_ids(rows)

    def picked(lane):
        chosen = (lanes == lane) | (lanes == lane + 3)
        return jnp.sum(jnp.where(chosen, extra, 0.0), axis=1, keepdims=True)

    scale_one = lax.rsqrt(picked(2) / width_all + norm_floor)
    proj_rows = proj_rows[:, :proj_width] * scale_one
    query = proj_rows[:, :query_size] * query_size ** (-0.5)
    key_vec = proj_rows[:, query_size : 2 * query_size]
    value = proj_rows[:, 2 * query_size : 2 * query_size + value_size]
    out_pre = proj_rows[:, 2 * query_size + value_size :]
    head_lane = lax.broadcasted_iota(jnp.int32, (1, heads_all), 1)
    bias = jnp.sum(jnp.where(head_lane == tp, bias_v[...], 0.0), axis=1, keepdims=True)
    log_input = picked(0) * scale_one
    forget_pre = picked(1) * scale_one + bias
    log_forget = -(jnp.maximum(-forget_pre, 0.0) + jnp.log1p(jnp.exp(-jnp.abs(forget_pre))))
    row_at = lax.broadcasted_iota(jnp.int32, (rows, rows), 0)
    same = row_at == lax.broadcasted_iota(jnp.int32, (rows, rows), 1)
    m_column = jnp.sum(jnp.where(same, m_v[...], 0.0), axis=1, keepdims=True)
    carried = log_forget + m_column
    m_next = jnp.maximum(carried, log_input)
    keep = jnp.exp(carried - m_next)
    admit = jnp.exp(log_input - m_next)
    n_next = keep * n_v[:, 0, :] + admit * key_vec
    denom = jnp.maximum(
        jnp.abs(jnp.sum(n_next * query, axis=1, keepdims=True)), jnp.exp(-m_next)
    )
    key_query = jnp.sum(key_vec * query, axis=1, keepdims=True)
    query_short = query.astype(bf16)
    query_rest = (query - query_short.astype(f32)).astype(bf16)
    row_ids = lax.broadcasted_iota(jnp.int32, (rows, value_size), 0)
    read = jnp.zeros((rows, value_size), f32)
    query_both = jnp.concatenate([query_short.astype(f32), query_rest.astype(f32)], axis=0).astype(bf16)
    for one in range(rows):
        product = dot_rows(query_both, c_short[one])
        read = jnp.where(row_ids == one, product[:rows] + product[rows:], read)
    admitted = admit * value
    numer = keep * read + admitted * key_query
    head_all[kv] = (jax.nn.sigmoid(out_pre) * numer / denom).astype(bf16)
    head_arrived, _, head_sent = exchange("kv", 1, lambda peer: head_all.at[kv], head_all)

    new_n[:, 0, :] = n_next
    new_m[...] = jnp.sum(jnp.where(same, m_next, 0.0), axis=0, keepdims=True)
    admitted_column = admitted.T
    for one in range(rows):
        new_c[one, 0] = (
            keep[one : one + 1, :] * c_v[one]
            + admitted_column[:, one : one + 1] * key_vec[one : one + 1, :]
        )

    load_out.wait()
    head_arrived()
    heads = head_all[...].astype(f32).reshape(batch, value_size).astype(bf16)
    attn_part = dot(heads, w_out_v[...])
    attn_send[...] = attn_part.reshape(tp_n, tp_rows, width).astype(bf16)
    _, attn_total, attn_sent = exchange("tp", 0, lambda peer: attn_send.at[peer], attn_recv)
    own_rows = pl.ds(pl.multiple_of(tp * tp_rows, tp_rows), tp_rows)
    attn_mix = attn_total(attn_send[tp].astype(f32))
    mid_all[tp] = (tok_v[own_rows, :].astype(f32) + attn_mix).astype(bf16)
    mid_arrived, _, mid_sent = exchange("tp", 1, lambda peer: mid_all.at[tp], mid_all)
    for copy in load_ff:
        copy.wait()
    mid_arrived()

    mid_float = mid_all[...].astype(f32).reshape(batch, width)
    squares_two = jnp.sum(mid_float * mid_float, axis=1, keepdims=True)
    normed_two = (mid_float * gain_two_v[...]).astype(bf16)
    lanes = lane_ids(batch)
    squares_short = squares_two.astype(bf16).astype(f32)
    extra = jnp.where(
        lanes == 0, squares_short, jnp.where(lanes == 1, squares_two - squares_short, 0.0)
    )
    ff_send[:, :, pl.ds(2 * ff_pad, LANES)] = extra.reshape(kv_n, rows, LANES).astype(bf16)
    for base, weight in ((0, w_gateff_v), (ff_pad, w_upff_v)):
        for at in range(0, ff, step):
            columns = min(step, ff - at)
            part = dot_rows(normed_two, weight[pl.ds(at, columns), :])
            ff_send[:, :, pl.ds(base + at, columns)] = part.reshape(kv_n, rows, columns).astype(bf16)
    _, ff_total, ff_sent = exchange("kv", 2, lambda peer: ff_send.at[peer], ff_recv)
    ff_rows = ff_total(ff_send[kv].astype(f32))
    rows_two = jnp.sum(ff_rows[:, 2 * ff_pad :], axis=1, keepdims=True)
    scale_two = lax.rsqrt(rows_two / width_all + norm_floor)
    gate_ff = ff_rows[:, :ff] * scale_two
    up_ff = ff_rows[:, ff_pad : ff_pad + ff] * scale_two
    hidden_all[kv] = (gate_ff / (1.0 + jnp.exp(-gate_ff)) * up_ff).astype(bf16)
    hidden_arrived, _, hidden_sent = exchange("kv", 3, lambda peer: hidden_all.at[kv], hidden_all)

    load_down.wait()
    hidden_arrived()
    hidden = hidden_all[...].astype(f32).reshape(batch, ff).astype(bf16)
    down_part = dot(hidden, w_down_v[...])
    down_send[...] = down_part.reshape(tp_n, tp_rows, width).astype(bf16)
    _, down_total, down_sent = exchange("tp", 2, lambda peer: down_send.at[peer], down_recv)
    down_sum = down_total(down_send[tp].astype(f32))
    mixed[tp] = (mid_all[tp].astype(f32) + down_sum).astype(bf16)
    mixed_arrived, _, mixed_sent = exchange("tp", 3, lambda peer: mixed.at[tp], mixed)
    for sent in (proj_sent, head_sent, attn_sent, mid_sent, ff_sent, hidden_sent, down_sent):
        sent()
    mixed_arrived()
    mixed_sent()


def write_out(count, *refs):
    sources, targets, sem = refs[:count], refs[count : 2 * count], refs[-1]
    copies = [
        pltpu.make_async_copy(source, target, sem.at[place])
        for place, (source, target) in enumerate(zip(sources, targets))
    ]
    for copy in copies:
        copy.start()
    for copy in copies:
        copy.wait()


def solution(mesh):
    kv_n, tp_n = mesh.shape["kv"], mesh.shape["tp"]

    def per_device(*args):
        args = list(args)
        for place in (1, 7, 12):
            args[place] = args[place].reshape(1, -1)
        for place in (6, 10, 13, 14):
            args[place] = args[place].T
        tokens, w_query, w_value, state_c, w_gateff = (args[i] for i in (0, 2, 4, 8, 13))
        batch, width = tokens.shape
        rows, tp_rows = batch // kv_n, batch // tp_n
        value_size, query_size = state_c.shape[2:]
        ff = w_gateff.shape[0]
        ff_pad = up_to_lanes(ff)
        proj_width = 2 * query_size + 2 * value_size
        heads_all = args[7].shape[1]
        V = pltpu.VMEM
        scratch = [
            V((batch, width), bf16),
            V((1, width), f32),
            V((width, proj_width), bf16),
            V((2 * heads_all, width), bf16),
            V((1, heads_all), f32),
            V((rows, value_size, query_size), f32),
            V((rows, 1, query_size), f32),
            V((1, rows), f32),
            V((value_size, width), bf16),
            V((1, width), f32),
            V((ff, width), bf16),
            V((ff, width), bf16),
            V((ff, width), bf16),
            V((rows, value_size, query_size), bf16),
            V((kv_n, rows, proj_width + LANES), bf16),
            V((kv_n, rows, proj_width + LANES), bf16),
            V((kv_n, rows, value_size), bf16),
            V((tp_n, tp_rows, width), bf16),
            V((tp_n, tp_rows, width), bf16),
            V((tp_n, tp_rows, width), bf16),
            V((kv_n, rows, 2 * ff_pad + LANES), bf16),
            V((kv_n, rows, 2 * ff_pad + LANES), bf16),
            V((kv_n, rows, ff), bf16),
            V((tp_n, tp_rows, width), bf16),
            V((tp_n, tp_rows, width), bf16),
            pltpu.SemaphoreType.DMA((16,)),
            pltpu.SemaphoreType.DMA((4, kv_n)),
            pltpu.SemaphoreType.DMA((4, kv_n)),
            pltpu.SemaphoreType.DMA((4, tp_n)),
            pltpu.SemaphoreType.DMA((4, tp_n)),
        ]
        anywhere = pl.BlockSpec(memory_space=pl.ANY)
        inside = pl.BlockSpec(memory_space=pltpu.VMEM)
        results = (
            ((tp_n, tp_rows, width), bf16),
            (state_c.shape, f32),
            (args[9].shape, f32),
            (args[10].shape, f32),
        )
        outs = pl.pallas_call(
            functools.partial(layer, kv_n, tp_n),
            out_shape=tuple(V(shape, dtype) for shape, dtype in results),
            in_specs=[anywhere] * len(args),
            out_specs=(inside,) * 4,
            scratch_shapes=scratch,
            compiler_params=pltpu.CompilerParams(
                collective_id=0, has_side_effects=True, vmem_limit_bytes=58 * 1024 * 1024
            ),
        )(*args)
        outs = pl.pallas_call(
            functools.partial(write_out, len(outs)),
            out_shape=tuple(jax.ShapeDtypeStruct(shape, dtype) for shape, dtype in results),
            in_specs=[inside] * len(outs),
            out_specs=(anywhere,) * len(outs),
            scratch_shapes=[pltpu.SemaphoreType.DMA((len(outs),))],
            compiler_params=pltpu.CompilerParams(vmem_limit_bytes=1024 * 1024),
        )(*outs)
        return (outs[0].reshape(batch, width), outs[1], outs[2], outs[3].T)

    placed = (
        P(None, "kv"),
        P("kv"),
        P("kv", "tp"),
        P("kv", "tp"),
        P("kv", "tp"),
        P("kv", "tp"),
        P(),
        P(),
        P("kv", "tp", None, None),
        P("kv", "tp", None),
        P("kv", "tp"),
        P("tp", "kv"),
        P("kv"),
        P("kv", "tp"),
        P("kv", "tp"),
        P("tp", "kv"),
    )
    return jax.shard_map(
        per_device,
        mesh=mesh,
        in_specs=placed,
        out_specs=(P(None, "kv"), P("kv", "tp", None, None), P("kv", "tp", None), P("kv", "tp")),
        check_vma=False,
    )
```

```python
import functools

import jax
import jax.numpy as jnp
from jax import lax
from jax.experimental import pallas as pl
from jax.experimental.pallas import tpu as pltpu
from jax.sharding import PartitionSpec as P

MESH = pl.DeviceIdType.MESH
norm_floor = 1e-05
f32 = jnp.float32
bf16 = jnp.bfloat16
LANES = 128


def up_to_lanes(length):
    return (length + LANES - 1) // LANES * LANES


def dot(a, b):
    return jnp.dot(a, b, preferred_element_type=f32)


def dot_rows(a, b):
    return lax.dot_general(a, b, (((1,), (1,)), ((), ())), preferred_element_type=f32)


def lane_ids(rows):
    return lax.broadcasted_iota(jnp.int32, (rows, LANES), 1)


def layer(
    kv_n,
    tp_n,
    tokens,
    attn_gain,
    w_query,
    w_key,
    w_value,
    w_outgate,
    w_gates,
    forget_bias,
    state_c,
    state_n,
    state_m,
    w_output,
    mlp_gain,
    w_gateff,
    w_upff,
    w_downff,
    mixed,
    new_c,
    new_n,
    new_m,
    tok_v,
    gain_one_v,
    w_proj_v,
    w_gates_v,
    bias_v,
    c_v,
    n_v,
    m_v,
    w_out_v,
    gain_two_v,
    w_gateff_v,
    w_upff_v,
    w_down_v,
    c_short,
    proj_send,
    proj_recv,
    head_all,
    attn_send,
    attn_recv,
    mid_all,
    ff_send,
    ff_recv,
    hidden_all,
    down_send,
    down_recv,
    in_sem,
    kv_send_sem,
    kv_recv_sem,
    tp_send_sem,
    tp_recv_sem,
):
    kv = lax.axis_index("kv")
    tp = lax.axis_index("tp")
    _, rows, width = tok_v.shape
    batch = kv_n * rows
    width_all = width * kv_n
    heads_all = bias_v.shape[1]
    value_size, query_size = c_v.shape[1:]
    proj_width = w_proj_v.shape[1]
    ff = w_gateff_v.shape[0]
    ff_pad = up_to_lanes(ff)

    side = 4
    near = {0: 0, 1: 1, 2: 2, 3: 1}
    kv_z, kv_y = kv // side, lax.rem(kv, side)
    tp_x, tp_core = tp // 2, lax.rem(tp, 2)

    def far_first(offsets):
        return sorted(offsets, key=lambda offset: -near[offset[0]] - near[offset[1]])

    square = [(a, b) for a in range(side) for b in range(side)]
    even = far_first([offset for offset in square if sum(offset) % 2 == 0])
    odd = far_first([offset for offset in square if sum(offset) % 2 == 1])
    around = far_first([offset for offset in square if offset != (0, 0)])
    tp_around = sorted([(a, b) for a in range(side) for b in range(2) if a or b], key=lambda at: -near[at[0]])

    def kv_peer(first, second):
        return lax.rem(kv_z + first, side) * side + lax.rem(kv_y + second, side)

    def tp_peer(first, second):
        return lax.rem(tp_x + first, side) * 2 + lax.rem(tp_core + second, 2)

    def block(group, place):
        first = place // 2
        return first * side + 2 * (place % 2) + (first + group) % 2

    parity = lax.rem(kv_z + kv_y, 2)

    barrier = pltpu.get_barrier_semaphore()

    def greet_kv(step, carry):
        pl.semaphore_signal(
            barrier, inc=1, device_id={"kv": lax.rem(kv + step, kv_n)}, device_id_type=MESH
        )
        return carry

    def greet_tp(step, carry):
        pl.semaphore_signal(
            barrier, inc=1, device_id={"tp": lax.rem(tp + step, tp_n)}, device_id_type=MESH
        )
        return carry

    lax.fori_loop(1, kv_n, greet_kv, 0)
    lax.fori_loop(1, tp_n, greet_tp, 0)

    loads = []

    def load(source, target):
        copy = pltpu.make_async_copy(source, target, in_sem.at[len(loads)])
        copy.start()
        loads.append(copy)
        return copy

    first = [load(tokens, tok_v), load(attn_gain, gain_one_v)]
    at = 0
    for weight in (w_query, w_key, w_value, w_outgate):
        columns = weight.shape[1]
        first.append(load(weight, w_proj_v.at[:, pl.ds(at, columns)]))
        at += columns
    first.append(load(w_gates.at[:, pl.ds(pl.multiple_of(kv * width, width), width)], w_gates_v))
    load_c = load(state_c.at[:, 0], c_v)
    load_cell = [load(state_n, n_v), load(state_m, m_v), load(forget_bias, bias_v)]
    load_out = load(w_output, w_out_v)
    load_ff = [load(mlp_gain, gain_two_v), load(w_gateff, w_gateff_v), load(w_upff, w_upff_v)]
    load_down = load(w_downff, w_down_v)

    def kv_copy(phase, source, target, peer, origin):
        return pltpu.make_async_remote_copy(
            src_ref=source,
            dst_ref=target,
            send_sem=kv_send_sem.at[phase, peer],
            recv_sem=kv_recv_sem.at[phase, origin],
            device_id={"kv": peer},
            device_id_type=MESH,
        )

    def tp_copy(phase, source, target, peer, origin):
        return pltpu.make_async_remote_copy(
            src_ref=source,
            dst_ref=target,
            send_sem=tp_send_sem.at[phase, peer],
            recv_sem=tp_recv_sem.at[phase, origin],
            device_id={"tp": peer},
            device_id_type=MESH,
        )

    unsent = []

    def scatter_group(phase, group, send, recv):
        mine = lax.rem(parity + group, 2) == 0
        for at_even, at_odd in zip(even, odd):
            peer = kv_peer(
                jnp.where(mine, at_even[0], at_odd[0]), jnp.where(mine, at_even[1], at_odd[1])
            )
            copy = kv_copy(phase, send.at[peer], recv.at[kv], peer, kv)
            if at_even == (0, 0):
                pl.when(jnp.logical_not(mine))(copy.start)
            else:
                copy.start()

    def scatter_total(phase, send, recv):
        def add(step, carry):
            peer = lax.rem(kv + step, kv_n)
            kv_copy(phase, send.at[peer], recv.at[peer], peer, peer).wait_recv()
            return carry + recv[peer].astype(f32)

        def sent(step, carry):
            peer = lax.rem(kv + step, kv_n)
            kv_copy(phase, send.at[peer], recv.at[kv], peer, kv).wait_send()
            return carry

        unsent.append((kv_n, sent))
        return lax.fori_loop(1, kv_n, add, send[kv].astype(f32))

    def gather_start(phase, blocks):
        for offset in around:
            peer = kv_peer(*offset)
            kv_copy(phase, blocks.at[kv], blocks.at[kv], peer, kv).start()

        def sent(step, carry):
            peer = lax.rem(kv + step, kv_n)
            kv_copy(phase, blocks.at[kv], blocks.at[kv], peer, kv).wait_send()
            return carry

        unsent.append((kv_n, sent))

    def gathered(phase, group, blocks):
        for place in range(tp_n):
            peer = block(group, place)
            copy = kv_copy(phase, blocks.at[peer], blocks.at[peer], peer, peer)
            pl.when(kv != peer)(copy.wait_recv)
        parts = [blocks[block(group, place)].astype(f32) for place in range(tp_n)]
        return jnp.concatenate(parts, axis=0).astype(bf16)

    def tp_sent(phase, source_of, target):
        def sent(step, carry):
            peer = lax.rem(tp + step, tp_n)
            tp_copy(phase, source_of(peer), target, peer, tp).wait_send()
            return carry

        unsent.append((tp_n, sent))

    def sum_start(phase, group, part, send, recv):
        for place in range(tp_n):
            send[block(group, place)] = part[place * rows : (place + 1) * rows].astype(bf16)
        for offset in tp_around:
            peer = tp_peer(*offset)
            tp_copy(phase, send.at[block(group, peer)], recv.at[group, tp], peer, tp).start()
        tp_sent(phase, lambda peer: send.at[block(group, peer)], recv.at[group, tp])

    def sum_total(phase, group, send, recv):
        total = send[block(group, tp)].astype(f32)
        for offset in reversed(tp_around):
            peer = tp_peer(*offset)
            tp_copy(phase, send.at[block(group, tp)], recv.at[group, peer], peer, peer).wait_recv()
            total = total + recv[group, peer].astype(f32)
        return total

    def share_start(phase, group, blocks):
        at = blocks.at[block(group, tp)]
        for offset in tp_around:
            tp_copy(phase, at, at, tp_peer(*offset), tp).start()
        tp_sent(phase, lambda peer: at, at)

    def shared(phase, group, blocks):
        for offset in reversed(tp_around):
            peer = tp_peer(*offset)
            at = blocks.at[block(group, peer)]
            tp_copy(phase, at, at, peer, peer).wait_recv()

    for copy in first:
        copy.wait()
    tok_float = tok_v[...].astype(f32).reshape(batch, width)
    squares_one = jnp.sum(tok_float * tok_float, axis=1, keepdims=True)
    normed_one = (tok_float * gain_one_v[...]).astype(bf16)
    lanes = lane_ids(batch)
    gate_row = lax.broadcasted_iota(jnp.int32, (LANES, 2 * heads_all), 1)
    gate_lane = lax.broadcasted_iota(jnp.int32, (LANES, 2 * heads_all), 0)
    wanted = jnp.where(
        (gate_lane == 0) | (gate_lane == 3),
        tp,
        jnp.where((gate_lane == 1) | (gate_lane == 4), heads_all + tp, -1),
    )
    pick = jnp.where(gate_row == wanted, 1.0, 0.0).astype(bf16)
    gate_weight = dot(pick, w_gates_v[...]).astype(bf16)
    extra = dot_rows(normed_one, gate_weight)
    extra = jnp.where((lanes == 2) | (lanes == 5), squares_one, extra)
    extra_short = extra.astype(bf16).astype(f32)
    extra = jnp.where(lanes < 3, extra_short, extra - extra_short)
    proj_send[:, :, pl.ds(proj_width, LANES)] = extra.reshape(kv_n, rows, LANES).astype(bf16)
    step = 512
    for at in range(0, proj_width, step):
        part = dot(normed_one, w_proj_v[:, pl.ds(at, step)])
        proj_send[:, :, pl.ds(at, step)] = part.reshape(kv_n, rows, step).astype(bf16)

    pl.semaphore_wait(barrier, kv_n + tp_n - 2)
    for group in range(2):
        scatter_group(0, group, proj_send, proj_recv)

    load_c.wait()
    for one in range(rows):
        c_short[one] = c_v[one].astype(bf16)
    for copy in load_cell:
        copy.wait()

    proj_rows = scatter_total(0, proj_send, proj_recv)
    extra = proj_rows[:, proj_width:]
    lanes = lane_ids(rows)

    def picked(lane):
        chosen = (lanes == lane) | (lanes == lane + 3)
        return jnp.sum(jnp.where(chosen, extra, 0.0), axis=1, keepdims=True)

    scale_one = lax.rsqrt(picked(2) / width_all + norm_floor)
    proj_rows = proj_rows[:, :proj_width] * scale_one
    query = proj_rows[:, :query_size] * query_size ** (-0.5)
    key_vec = proj_rows[:, query_size : 2 * query_size]
    value = proj_rows[:, 2 * query_size : 2 * query_size + value_size]
    out_pre = proj_rows[:, 2 * query_size + value_size :]
    head_lane = lax.broadcasted_iota(jnp.int32, (1, heads_all), 1)
    bias = jnp.sum(jnp.where(head_lane == tp, bias_v[...], 0.0), axis=1, keepdims=True)
    log_input = picked(0) * scale_one
    forget_pre = picked(1) * scale_one + bias
    log_forget = -(jnp.maximum(-forget_pre, 0.0) + jnp.log1p(jnp.exp(-jnp.abs(forget_pre))))
    row_at = lax.broadcasted_iota(jnp.int32, (rows, rows), 0)
    same = row_at == lax.broadcasted_iota(jnp.int32, (rows, rows), 1)
    m_column = jnp.sum(jnp.where(same, m_v[...], 0.0), axis=1, keepdims=True)
    carried = log_forget + m_column
    m_next = jnp.maximum(carried, log_input)
    keep = jnp.exp(carried - m_next)
    admit = jnp.exp(log_input - m_next)
    n_next = keep * n_v[:, 0, :] + admit * key_vec
    denom = jnp.maximum(
        jnp.abs(jnp.sum(n_next * query, axis=1, keepdims=True)), jnp.exp(-m_next)
    )
    key_query = jnp.sum(key_vec * query, axis=1, keepdims=True)
    query_short = query.astype(bf16)
    query_rest = (query - query_short.astype(f32)).astype(bf16)
    row_ids = lax.broadcasted_iota(jnp.int32, (rows, value_size), 0)
    read = jnp.zeros((rows, value_size), f32)
    query_both = jnp.concatenate([query_short.astype(f32), query_rest.astype(f32)], axis=0).astype(bf16)
    for one in range(rows):
        product = dot_rows(query_both, c_short[one])
        read = jnp.where(row_ids == one, product[:rows] + product[rows:], read)
    admitted = admit * value
    numer = keep * read + admitted * key_query
    head_all[kv] = (jax.nn.sigmoid(out_pre) * numer / denom).astype(bf16)
    gather_start(1, head_all)

    new_n[:, 0, :] = n_next
    new_m[...] = jnp.sum(jnp.where(same, m_next, 0.0), axis=0, keepdims=True)
    admitted_column = admitted.T
    for one in range(rows):
        new_c[one, 0] = (
            keep[one : one + 1, :] * c_v[one]
            + admitted_column[:, one : one + 1] * key_vec[one : one + 1, :]
        )

    load_out.wait()
    for group in range(2):
        heads = gathered(1, group, head_all)
        sum_start(group, group, dot(heads, w_out_v[...]), attn_send, attn_recv)
    for group in range(2):
        own = block(group, tp)
        attn_mix = sum_total(group, group, attn_send, attn_recv)
        mid_all[own] = (tok_v[own].astype(f32) + attn_mix).astype(bf16)
        share_start(2 + group, group, mid_all)
    for copy in load_ff:
        copy.wait()

    for group in range(2):
        shared(2 + group, group, mid_all)
        parts = [mid_all[block(group, place)].astype(f32) for place in range(tp_n)]
        mid_float = jnp.concatenate(parts, axis=0)
        squares_two = jnp.sum(mid_float * mid_float, axis=1, keepdims=True)
        normed_two = (mid_float * gain_two_v[...]).astype(bf16)
        lanes = lane_ids(tp_n * rows)
        squares_short = squares_two.astype(bf16).astype(f32)
        extra = jnp.where(
            lanes == 0, squares_short, jnp.where(lanes == 1, squares_two - squares_short, 0.0)
        )
        pieces = [(2 * ff_pad, LANES, extra)]
        for base, weight in ((0, w_gateff_v), (ff_pad, w_upff_v)):
            for at in range(0, ff, step):
                columns = min(step, ff - at)
                pieces.append(
                    (base + at, columns, dot_rows(normed_two, weight[pl.ds(at, columns), :]))
                )
        for at, columns, part in pieces:
            for place in range(tp_n):
                ff_send[block(group, place), :, pl.ds(at, columns)] = part[
                    place * rows : (place + 1) * rows
                ].astype(bf16)
        scatter_group(2, group, ff_send, ff_recv)
    ff_rows = scatter_total(2, ff_send, ff_recv)
    rows_two = jnp.sum(ff_rows[:, 2 * ff_pad :], axis=1, keepdims=True)
    scale_two = lax.rsqrt(rows_two / width_all + norm_floor)
    gate_ff = ff_rows[:, :ff] * scale_two
    up_ff = ff_rows[:, ff_pad : ff_pad + ff] * scale_two
    hidden_all[kv] = (gate_ff / (1.0 + jnp.exp(-gate_ff)) * up_ff).astype(bf16)
    gather_start(3, hidden_all)

    load_down.wait()
    for group in range(2):
        hidden = gathered(3, group, hidden_all)
        sum_start(4 + group, group, dot(hidden, w_down_v[...]), down_send, down_recv)
    for group in range(2):
        own = block(group, tp)
        down_sum = sum_total(4 + group, group, down_send, down_recv)
        mixed[own] = (mid_all[own].astype(f32) + down_sum).astype(bf16)
        share_start(6 + group, group, mixed)
    for count, sent in unsent:
        lax.fori_loop(1, count, sent, 0)
    for group in range(2):
        shared(6 + group, group, mixed)


def write_out(count, *refs):
    sources, targets, sem = refs[:count], refs[count : 2 * count], refs[-1]
    copies = [
        pltpu.make_async_copy(source, target, sem.at[place])
        for place, (source, target) in enumerate(zip(sources, targets))
    ]
    for copy in copies:
        copy.start()
    for copy in copies:
        copy.wait()


def solution(mesh):
    kv_n, tp_n = mesh.shape["kv"], mesh.shape["tp"]

    def per_device(*args):
        args = list(args)
        for place in (1, 7, 12):
            args[place] = args[place].reshape(1, -1)
        for place in (6, 10, 13, 14):
            args[place] = args[place].T
        tokens, w_query, w_value, state_c, w_gateff = (args[i] for i in (0, 2, 4, 8, 13))
        batch, width = tokens.shape
        rows = batch // kv_n
        args[0] = tokens.reshape(kv_n, rows, width)
        value_size, query_size = state_c.shape[2:]
        ff = w_gateff.shape[0]
        ff_pad = up_to_lanes(ff)
        proj_width = 2 * query_size + 2 * value_size
        heads_all = args[7].shape[1]
        V = pltpu.VMEM
        scratch = [
            V((kv_n, rows, width), bf16),
            V((1, width), f32),
            V((width, proj_width), bf16),
            V((2 * heads_all, width), bf16),
            V((1, heads_all), f32),
            V((rows, value_size, query_size), f32),
            V((rows, 1, query_size), f32),
            V((1, rows), f32),
            V((value_size, width), bf16),
            V((1, width), f32),
            V((ff, width), bf16),
            V((ff, width), bf16),
            V((ff, width), bf16),
            V((rows, value_size, query_size), bf16),
            V((kv_n, rows, proj_width + LANES), bf16),
            V((kv_n, rows, proj_width + LANES), bf16),
            V((kv_n, rows, value_size), bf16),
            V((kv_n, rows, width), bf16),
            V((2, tp_n, rows, width), bf16),
            V((kv_n, rows, width), bf16),
            V((kv_n, rows, 2 * ff_pad + LANES), bf16),
            V((kv_n, rows, 2 * ff_pad + LANES), bf16),
            V((kv_n, rows, ff), bf16),
            V((kv_n, rows, width), bf16),
            V((2, tp_n, rows, width), bf16),
            pltpu.SemaphoreType.DMA((16,)),
            pltpu.SemaphoreType.DMA((4, kv_n)),
            pltpu.SemaphoreType.DMA((4, kv_n)),
            pltpu.SemaphoreType.DMA((8, tp_n)),
            pltpu.SemaphoreType.DMA((8, tp_n)),
        ]
        anywhere = pl.BlockSpec(memory_space=pl.ANY)
        inside = pl.BlockSpec(memory_space=pltpu.VMEM)
        results = (
            ((kv_n, rows, width), bf16),
            (state_c.shape, f32),
            (args[9].shape, f32),
            (args[10].shape, f32),
        )
        outs = pl.pallas_call(
            functools.partial(layer, kv_n, tp_n),
            out_shape=tuple(V(shape, dtype) for shape, dtype in results),
            in_specs=[anywhere] * len(args),
            out_specs=(inside,) * 4,
            scratch_shapes=scratch,
            compiler_params=pltpu.CompilerParams(
                collective_id=0, has_side_effects=True, vmem_limit_bytes=58 * 1024 * 1024
            ),
        )(*args)
        outs = pl.pallas_call(
            functools.partial(write_out, len(outs)),
            out_shape=tuple(jax.ShapeDtypeStruct(shape, dtype) for shape, dtype in results),
            in_specs=[inside] * len(outs),
            out_specs=(anywhere,) * len(outs),
            scratch_shapes=[pltpu.SemaphoreType.DMA((len(outs),))],
            compiler_params=pltpu.CompilerParams(vmem_limit_bytes=1024 * 1024),
        )(*outs)
        return (outs[0].reshape(batch, width), outs[1], outs[2], outs[3].T)

    placed = (
        P(None, "kv"),
        P("kv"),
        P("kv", "tp"),
        P("kv", "tp"),
        P("kv", "tp"),
        P("kv", "tp"),
        P(),
        P(),
        P("kv", "tp", None, None),
        P("kv", "tp", None),
        P("kv", "tp"),
        P("tp", "kv"),
        P("kv"),
        P("kv", "tp"),
        P("kv", "tp"),
        P("tp", "kv"),
    )
    return jax.shard_map(
        per_device,
        mesh=mesh,
        in_specs=placed,
        out_specs=(P(None, "kv"), P("kv", "tp", None, None), P("kv", "tp", None), P("kv", "tp")),
        check_vma=False,
    )
```

```python
import functools

import jax
import jax.numpy as jnp
from jax import lax
from jax.experimental import pallas as pl
from jax.experimental.pallas import tpu as pltpu
from jax.sharding import PartitionSpec as P

MESH = pl.DeviceIdType.MESH
norm_floor = 1e-05
f32 = jnp.float32
bf16 = jnp.bfloat16
LANES = 128


def up_to_lanes(length):
    return (length + LANES - 1) // LANES * LANES


def dot(a, b):
    return jnp.dot(a, b, preferred_element_type=f32)


def dot_rows(a, b):
    return lax.dot_general(a, b, (((1,), (1,)), ((), ())), preferred_element_type=f32)


def lane_ids(rows):
    return lax.broadcasted_iota(jnp.int32, (rows, LANES), 1)


def layer(
    kv_n,
    tp_n,
    tokens,
    attn_gain,
    w_query,
    w_key,
    w_value,
    w_outgate,
    w_gates,
    forget_bias,
    state_c,
    state_n,
    state_m,
    w_output,
    mlp_gain,
    w_gateff,
    w_upff,
    w_downff,
    mixed,
    new_c,
    new_n,
    new_m,
    tok_v,
    gain_one_v,
    w_proj_v,
    w_gates_v,
    bias_v,
    c_v,
    n_v,
    m_v,
    w_out_v,
    gain_two_v,
    w_gateff_v,
    w_upff_v,
    w_down_v,
    c_short,
    proj_send,
    proj_recv,
    head_all,
    part_f32,
    attn_swap,
    attn_swapped,
    attn_quads,
    mid_all,
    ff_send,
    ff_recv,
    hidden_all,
    down_swap,
    down_swapped,
    down_quads,
    in_sem,
    kv_send_sem,
    kv_recv_sem,
    tp_send_sem,
    tp_recv_sem,
):
    kv = lax.axis_index("kv")
    tp = lax.axis_index("tp")
    _, half, width = tok_v.shape
    batch = 2 * half
    rows = batch // kv_n
    width_all = width * kv_n
    heads_all = bias_v.shape[1]
    value_size, query_size = c_v.shape[1:]
    proj_width = w_proj_v.shape[1]
    ff, ff_pad = w_down_v.shape[0], w_gateff_v.shape[0]

    side = 4
    near = {0: 0, 1: 1, 2: 2, 3: 1}
    kv_z, kv_y = kv // side, lax.rem(kv, side)
    ring, core = tp // 2, lax.rem(tp, 2)
    partner = ring * 2 + (1 - core)
    around = [(a, b) for a in range(side) for b in range(side) if a or b]
    around.sort(key=lambda offset: -near[offset[0]] - near[offset[1]])

    def kv_peer(first, second):
        return lax.rem(kv_z + first, side) * side + lax.rem(kv_y + second, side)

    barrier = pltpu.get_barrier_semaphore()

    def greet_kv(step, carry):
        pl.semaphore_signal(
            barrier, inc=1, device_id={"kv": lax.rem(kv + step, kv_n)}, device_id_type=MESH
        )
        return carry

    def greet_tp(step, carry):
        pl.semaphore_signal(
            barrier, inc=1, device_id={"tp": lax.rem(tp + step, tp_n)}, device_id_type=MESH
        )
        return carry

    lax.fori_loop(1, kv_n, greet_kv, 0)
    lax.fori_loop(1, tp_n, greet_tp, 0)

    loads = []

    def load(source, target):
        copy = pltpu.make_async_copy(source, target, in_sem.at[len(loads)])
        copy.start()
        loads.append(copy)
        return copy

    first = [load(tokens, tok_v), load(attn_gain, gain_one_v)]
    at = 0
    for weight in (w_query, w_key, w_value, w_outgate):
        columns = weight.shape[1]
        first.append(load(weight, w_proj_v.at[:, pl.ds(at, columns)]))
        at += columns
    first.append(load(w_gates.at[:, pl.ds(pl.multiple_of(kv * width, width), width)], w_gates_v))
    load_c = load(state_c.at[:, 0], c_v)
    load_cell = [load(state_n, n_v), load(state_m, m_v), load(forget_bias, bias_v)]
    load_out = load(w_output, w_out_v)
    load_ff = [load(mlp_gain, gain_two_v), load(w_gateff, w_gateff_v.at[pl.ds(0, ff)]), load(w_upff, w_upff_v.at[pl.ds(0, ff)])]
    load_down = load(w_downff, w_down_v)

    def kv_copy(phase, source, target, peer, origin):
        return pltpu.make_async_remote_copy(
            src_ref=source,
            dst_ref=target,
            send_sem=kv_send_sem.at[phase, peer],
            recv_sem=kv_recv_sem.at[phase, origin],
            device_id={"kv": peer},
            device_id_type=MESH,
        )

    unsent = []

    def all_sent():
        for wait in unsent:
            wait()
        unsent.clear()

    def kv_sent(phase, source_of, target):
        def one(step, carry):
            peer = lax.rem(kv + step, kv_n)
            kv_copy(phase, source_of(peer), target, peer, kv).wait_send()
            return carry

        unsent.append(lambda: lax.fori_loop(1, kv_n, one, 0))

    def scatter_total(phase, send, recv):
        def add(step, carry):
            peer = lax.rem(kv + step, kv_n)
            kv_copy(phase, send.at[peer], recv.at[peer], peer, peer).wait_recv()
            return carry + recv[peer].astype(f32)

        kv_sent(phase, lambda peer: send.at[peer], recv.at[kv])
        return lax.fori_loop(1, kv_n, add, send[kv].astype(f32))

    def gather_start(phase, blocks):
        for offset in around:
            peer = kv_peer(*offset)
            kv_copy(phase, blocks.at[kv], blocks.at[kv], peer, kv).start()
        kv_sent(phase, lambda peer: blocks.at[kv], blocks.at[kv])

    def gathered(phase, blocks):
        def wait(step, carry):
            peer = lax.rem(kv + step, kv_n)
            kv_copy(phase, blocks.at[peer], blocks.at[peer], peer, peer).wait_recv()
            return carry

        lax.fori_loop(1, kv_n, wait, 0)
        return blocks[...].astype(f32).reshape(batch, blocks.shape[2]).astype(bf16)

    def tp_copy(place, source, target, peer):
        return pltpu.make_async_remote_copy(
            src_ref=source,
            dst_ref=target,
            send_sem=tp_send_sem.at[place],
            recv_sem=tp_recv_sem.at[place],
            device_id={"tp": peer},
            device_id_type=MESH,
        )

    def tp_total(first, part, part_f32, swap_send, swap_recv, quads):
        part_f32[...] = part.reshape(2, half, width)
        swap_send[...] = part_f32[1 - core].astype(bf16)
        swap = tp_copy(first, swap_send, swap_recv, partner)
        swap.start()
        swap.wait_recv()
        quads[ring] = (part_f32[core] + swap_recv[...].astype(f32)).astype(bf16)
        copies = []
        for offset in (2, 1, 3):
            peer = lax.rem(ring + offset, side) * 2 + core
            copies.append(tp_copy(first + offset, quads.at[ring], quads.at[ring], peer))
        for copy in copies:
            copy.start()
        all_sent()
        for offset in (3, 1, 2):
            at = quads.at[lax.rem(ring + side - offset, side)]
            tp_copy(first + offset, at, at, partner).wait_recv()
        unsent.append(swap.wait_send)
        unsent.extend(copy.wait_send for copy in copies)
        total = quads[0].astype(f32)
        for place in range(1, side):
            total = total + quads[place].astype(f32)
        return total

    def tp_share(place, halves):
        copy = tp_copy(place, halves.at[core], halves.at[core], partner)
        copy.start()
        unsent.append(copy.wait_send)
        other = halves.at[1 - core]
        return tp_copy(place, other, other, partner).wait_recv

    for copy in first:
        copy.wait()
    tok_float = tok_v[...].astype(f32).reshape(batch, width)
    squares_one = jnp.sum(tok_float * tok_float, axis=1, keepdims=True)
    normed_one = (tok_float * gain_one_v[...]).astype(bf16)
    lanes = lane_ids(batch)
    gate_row = lax.broadcasted_iota(jnp.int32, (LANES, 2 * heads_all), 1)
    gate_lane = lax.broadcasted_iota(jnp.int32, (LANES, 2 * heads_all), 0)
    wanted = jnp.where(
        (gate_lane == 0) | (gate_lane == 3),
        tp,
        jnp.where((gate_lane == 1) | (gate_lane == 4), heads_all + tp, -1),
    )
    pick = jnp.where(gate_row == wanted, 1.0, 0.0).astype(bf16)
    gate_weight = dot(pick, w_gates_v[...]).astype(bf16)
    extra = dot_rows(normed_one, gate_weight)
    extra = jnp.where((lanes == 2) | (lanes == 5), squares_one, extra)
    extra_short = extra.astype(bf16).astype(f32)
    extra = jnp.where(lanes < 3, extra_short, extra - extra_short)
    proj_send[:, :, pl.ds(proj_width, LANES)] = extra.reshape(kv_n, rows, LANES).astype(bf16)
    step = 512
    for at in range(0, proj_width, step):
        part = dot(normed_one, w_proj_v[:, pl.ds(at, step)])
        proj_send[:, :, pl.ds(at, step)] = part.reshape(kv_n, rows, step).astype(bf16)

    pl.semaphore_wait(barrier, kv_n + tp_n - 2)
    for offset in around:
        peer = kv_peer(*offset)
        kv_copy(0, proj_send.at[peer], proj_recv.at[kv], peer, kv).start()

    load_c.wait()
    for one in range(rows):
        c_short[one] = c_v[one].astype(bf16)
    for copy in load_cell:
        copy.wait()

    proj_rows = scatter_total(0, proj_send, proj_recv)
    extra = proj_rows[:, proj_width:]
    lanes = lane_ids(rows)

    def picked(lane):
        chosen = (lanes == lane) | (lanes == lane + 3)
        return jnp.sum(jnp.where(chosen, extra, 0.0), axis=1, keepdims=True)

    scale_one = lax.rsqrt(picked(2) / width_all + norm_floor)
    proj_rows = proj_rows[:, :proj_width] * scale_one
    query = proj_rows[:, :query_size] * query_size ** (-0.5)
    key_vec = proj_rows[:, query_size : 2 * query_size]
    value = proj_rows[:, 2 * query_size : 2 * query_size + value_size]
    out_pre = proj_rows[:, 2 * query_size + value_size :]
    head_lane = lax.broadcasted_iota(jnp.int32, (1, heads_all), 1)
    bias = jnp.sum(jnp.where(head_lane == tp, bias_v[...], 0.0), axis=1, keepdims=True)
    log_input = picked(0) * scale_one
    forget_pre = picked(1) * scale_one + bias
    log_forget = -(jnp.maximum(-forget_pre, 0.0) + jnp.log1p(jnp.exp(-jnp.abs(forget_pre))))
    row_at = lax.broadcasted_iota(jnp.int32, (rows, rows), 0)
    same = row_at == lax.broadcasted_iota(jnp.int32, (rows, rows), 1)
    m_column = jnp.sum(jnp.where(same, m_v[...], 0.0), axis=1, keepdims=True)
    carried = log_forget + m_column
    m_next = jnp.maximum(carried, log_input)
    keep = jnp.exp(carried - m_next)
    admit = jnp.exp(log_input - m_next)
    n_next = keep * n_v[:, 0, :] + admit * key_vec
    denom = jnp.maximum(
        jnp.abs(jnp.sum(n_next * query, axis=1, keepdims=True)), jnp.exp(-m_next)
    )
    key_query = jnp.sum(key_vec * query, axis=1, keepdims=True)
    query_short = query.astype(bf16)
    query_rest = (query - query_short.astype(f32)).astype(bf16)
    row_ids = lax.broadcasted_iota(jnp.int32, (rows, value_size), 0)
    read = jnp.zeros((rows, value_size), f32)
    query_both = jnp.concatenate([query_short.astype(f32), query_rest.astype(f32)], axis=0).astype(bf16)
    for one in range(rows):
        product = dot_rows(query_both, c_short[one])
        read = jnp.where(row_ids == one, product[:rows] + product[rows:], read)
    admitted = admit * value
    numer = keep * read + admitted * key_query
    head_all[kv] = (jax.nn.sigmoid(out_pre) * numer / denom).astype(bf16)
    gather_start(1, head_all)

    new_n[:, 0, :] = n_next
    new_m[...] = jnp.sum(jnp.where(same, m_next, 0.0), axis=0, keepdims=True)
    admitted_column = admitted.T
    for one in range(rows):
        new_c[one, 0] = (
            keep[one : one + 1, :] * c_v[one]
            + admitted_column[:, one : one + 1] * key_vec[one : one + 1, :]
        )

    load_out.wait()
    heads = gathered(1, head_all)
    attn_part = dot(heads, w_out_v[...])
    attn_mix = tp_total(0, attn_part, part_f32, attn_swap, attn_swapped, attn_quads)
    mid_all[core] = (tok_v[core].astype(f32) + attn_mix).astype(bf16)
    mid_arrived = tp_share(4, mid_all)
    for copy in load_ff:
        copy.wait()

    lanes = lane_ids(half)
    for turn in range(2):
        at_half = core if turn == 0 else 1 - core
        if turn == 1:
            mid_arrived()
        mid_float = mid_all[at_half].astype(f32)
        squares_two = jnp.sum(mid_float * mid_float, axis=1, keepdims=True)
        normed_two = (mid_float * gain_two_v[...]).astype(bf16)
        squares_short = squares_two.astype(bf16).astype(f32)
        extra = jnp.where(lanes == LANES - 2, squares_short, squares_two - squares_short)
        for base, weight in ((0, w_gateff_v), (ff_pad, w_upff_v)):
            for at in range(0, ff_pad, step):
                columns = min(step, ff_pad - at)
                part = dot_rows(normed_two, weight[pl.ds(at, columns), :])
                if base == 0 and at + columns == ff_pad:
                    last = jnp.where(lanes < LANES - 2, part[:, columns - LANES :], extra)
                    part = jnp.concatenate([part[:, : columns - LANES], last], axis=1)
                part = part.reshape(kv_n // 2, rows, columns).astype(bf16)
                ff_send[pl.ds(at_half * (kv_n // 2), kv_n // 2), :, pl.ds(base + at, columns)] = part
        for second in (2, 1, 3, 0):
            for first in range(side // 2):
                peer = (at_half * (side // 2) + first) * side + lax.rem(kv_y + second, side)
                copy = kv_copy(2, ff_send.at[peer], ff_recv.at[kv], peer, kv)
                if second == 0:
                    pl.when(peer != kv)(copy.start)
                else:
                    copy.start()
    ff_rows = scatter_total(2, ff_send, ff_recv)
    rows_two = jnp.sum(ff_rows[:, ff_pad - 2 : ff_pad], axis=1, keepdims=True)
    scale_two = lax.rsqrt(rows_two / width_all + norm_floor)
    gate_ff = ff_rows[:, :ff] * scale_two
    up_ff = ff_rows[:, ff_pad : ff_pad + ff] * scale_two
    hidden_all[kv] = (gate_ff / (1.0 + jnp.exp(-gate_ff)) * up_ff).astype(bf16)
    gather_start(3, hidden_all)

    load_down.wait()
    hidden = gathered(3, hidden_all)
    down_part = dot(hidden, w_down_v[...])
    down_sum = tp_total(5, down_part, part_f32, down_swap, down_swapped, down_quads)
    mixed[core] = (mid_all[core].astype(f32) + down_sum).astype(bf16)
    mixed_arrived = tp_share(9, mixed)
    mixed_arrived()
    all_sent()


def write_out(count, *refs):
    pairs = list(zip(refs[:count], refs[count : 2 * count]))
    sem = refs[-1]
    source, target = pairs.pop(1)
    pairs += [(source.at[one], target.at[one]) for one in range(source.shape[0])]
    copies = [
        pltpu.make_async_copy(source, target, sem.at[place])
        for place, (source, target) in enumerate(pairs)
    ]
    for copy in copies:
        copy.start()
    for copy in copies:
        copy.wait()


def solution(mesh):
    kv_n, tp_n = mesh.shape["kv"], mesh.shape["tp"]

    def per_device(*args):
        args = list(args)
        for place in (1, 7, 12):
            args[place] = args[place].reshape(1, -1)
        for place in (6, 10, 13, 14):
            args[place] = args[place].T
        tokens, w_query, w_value, state_c, w_gateff = (args[i] for i in (0, 2, 4, 8, 13))
        batch, width = tokens.shape
        rows, half = batch // kv_n, batch // 2
        args[0] = tokens.reshape(2, half, width)
        value_size, query_size = state_c.shape[2:]
        ff = w_gateff.shape[0]
        ff_pad = up_to_lanes(ff)
        proj_width = 2 * query_size + 2 * value_size
        heads_all = args[7].shape[1]
        V = pltpu.VMEM
        scratch = [
            V((2, half, width), bf16),
            V((1, width), f32),
            V((width, proj_width), bf16),
            V((2 * heads_all, width), bf16),
            V((1, heads_all), f32),
            V((rows, value_size, query_size), f32),
            V((rows, 1, query_size), f32),
            V((1, rows), f32),
            V((value_size, width), bf16),
            V((1, width), f32),
            V((ff_pad, width), bf16),
            V((ff_pad, width), bf16),
            V((ff, width), bf16),
            V((rows, value_size, query_size), bf16),
            V((kv_n, rows, proj_width + LANES), bf16),
            V((kv_n, rows, proj_width + LANES), bf16),
            V((kv_n, rows, value_size), bf16),
            V((2, half, width), f32),
            V((half, width), bf16),
            V((half, width), bf16),
            V((tp_n // 2, half, width), bf16),
            V((2, half, width), bf16),
            V((kv_n, rows, 2 * ff_pad), bf16),
            V((kv_n, rows, 2 * ff_pad), bf16),
            V((kv_n, rows, ff), bf16),
            V((half, width), bf16),
            V((half, width), bf16),
            V((tp_n // 2, half, width), bf16),
            pltpu.SemaphoreType.DMA((16,)),
            pltpu.SemaphoreType.DMA((4, kv_n)),
            pltpu.SemaphoreType.DMA((4, kv_n)),
            pltpu.SemaphoreType.DMA((10,)),
            pltpu.SemaphoreType.DMA((10,)),
        ]
        anywhere = pl.BlockSpec(memory_space=pl.ANY)
        inside = pl.BlockSpec(memory_space=pltpu.VMEM)
        results = (
            ((2, half, width), bf16),
            (state_c.shape, f32),
            (args[9].shape, f32),
            (args[10].shape, f32),
        )
        outs = pl.pallas_call(
            functools.partial(layer, kv_n, tp_n),
            out_shape=tuple(V(shape, dtype) for shape, dtype in results),
            in_specs=[anywhere] * len(args),
            out_specs=(inside,) * 4,
            scratch_shapes=scratch,
            compiler_params=pltpu.CompilerParams(
                collective_id=0, has_side_effects=True, vmem_limit_bytes=58 * 1024 * 1024
            ),
        )(*args)
        outs = pl.pallas_call(
            functools.partial(write_out, len(outs)),
            out_shape=tuple(jax.ShapeDtypeStruct(shape, dtype) for shape, dtype in results),
            in_specs=[inside] * len(outs),
            out_specs=(anywhere,) * len(outs),
            scratch_shapes=[pltpu.SemaphoreType.DMA((len(outs) - 1 + rows,))],
            compiler_params=pltpu.CompilerParams(vmem_limit_bytes=1024 * 1024),
        )(*outs)
        return (outs[0].reshape(batch, width), outs[1], outs[2], outs[3].T)

    placed = (
        P(None, "kv"),
        P("kv"),
        P("kv", "tp"),
        P("kv", "tp"),
        P("kv", "tp"),
        P("kv", "tp"),
        P(),
        P(),
        P("kv", "tp", None, None),
        P("kv", "tp", None),
        P("kv", "tp"),
        P("tp", "kv"),
        P("kv"),
        P("kv", "tp"),
        P("kv", "tp"),
        P("tp", "kv"),
    )
    return jax.shard_map(
        per_device,
        mesh=mesh,
        in_specs=placed,
        out_specs=(P(None, "kv"), P("kv", "tp", None, None), P("kv", "tp", None), P("kv", "tp")),
        check_vma=False,
    )
```

```python
import functools

import jax
import jax.numpy as jnp
from jax import lax
from jax.experimental import pallas as pl
from jax.experimental.pallas import tpu as pltpu
from jax.sharding import PartitionSpec as P

MESH = pl.DeviceIdType.MESH
norm_floor = 1e-05
f32 = jnp.float32
bf16 = jnp.bfloat16
LANES = 128


def up_to_lanes(length):
    return (length + LANES - 1) // LANES * LANES


def dot(a, b):
    return jnp.dot(a, b, preferred_element_type=f32)


def dot_rows(a, b):
    return lax.dot_general(a, b, (((1,), (1,)), ((), ())), preferred_element_type=f32)


def lane_ids(rows):
    return lax.broadcasted_iota(jnp.int32, (rows, LANES), 1)


def layer(
    kv_n,
    tp_n,
    chunks,
    tokens,
    attn_gain,
    w_query,
    w_key,
    w_value,
    w_outgate,
    w_gates,
    forget_bias,
    state_c,
    state_n,
    state_m,
    w_output,
    mlp_gain,
    w_gateff,
    w_upff,
    w_downff,
    mixed,
    new_c,
    new_n,
    new_m,
    tok_v,
    gains_v,
    w_proj_v,
    w_gates_v,
    bias_v,
    c_v,
    n_v,
    m_v,
    w_out_v,
    w_ff_v,
    w_down_v,
    c_short,
    qk_send,
    qk_recv,
    vo_send,
    vo_recv,
    head_all,
    part_f32,
    attn_swap,
    attn_swapped,
    attn_quads,
    mid_all,
    ff_send_0,
    ff_recv_0,
    ff_send_1,
    ff_recv_1,
    hidden_0,
    hidden_1,
    down_swap,
    down_swapped,
    down_quads,
    in_sem,
    kv_send_sem,
    kv_recv_sem,
    tp_send_sem,
    tp_recv_sem,
):
    kv = lax.axis_index("kv")
    tp = lax.axis_index("tp")
    _, rows, width = tok_v.shape
    batch = kv_n * rows
    half = batch // 2
    places = kv_n // 2
    width_all = width * kv_n
    heads_all = bias_v.shape[1]
    value_size, query_size = c_v.shape[1:]
    qk_width = 2 * query_size
    vo_width = 2 * value_size

    side = 4
    near = {0: 0, 1: 1, 2: 2, 3: 1}
    kv_z, kv_y = kv // side, lax.rem(kv, side)
    ring, core = tp // 2, lax.rem(tp, 2)
    partner = ring * 2 + (1 - core)

    def far_first(offsets):
        return sorted(offsets, key=lambda offset: -near[offset[0]] - near[offset[1]])

    square = [(a, b) for a in range(side) for b in range(side)]
    around = far_first([offset for offset in square if offset != (0, 0)])
    even = far_first([offset for offset in square if sum(offset) % 2 == 0])
    odd = far_first([offset for offset in square if sum(offset) % 2 == 1])
    colour = lax.rem(kv_z + kv_y, 2)

    def kv_peer(first, second):
        return lax.rem(kv_z + first, side) * side + lax.rem(kv_y + second, side)

    barrier = pltpu.get_barrier_semaphore()

    for offset in around:
        pl.semaphore_signal(
            barrier, inc=1, device_id={"kv": kv_peer(*offset)}, device_id_type=MESH
        )
    tp_peers = [partner] + [lax.rem(ring + offset, side) * 2 + core for offset in (1, 2, 3)]
    for peer in tp_peers:
        pl.semaphore_signal(barrier, inc=1, device_id={"tp": peer}, device_id_type=MESH)

    loads = []

    def load(*pairs, whole=None):
        sem = in_sem.at[len(loads)]
        loads.append(sem)
        for source, target in pairs:
            pltpu.make_async_copy(source, target, sem).start()
        whole = pairs[0][1] if whole is None else whole
        return pltpu.make_async_copy(whole, whole, sem).wait

    wait_tok = load((tokens, tok_v))
    wait_gains = load((attn_gain, gains_v.at[0]), (mlp_gain, gains_v.at[1]), whole=gains_v)
    wait_gates = load((w_gates.at[:, pl.ds(pl.multiple_of(kv * width, width), width)], w_gates_v))
    pairs, at = [], 0
    for weight in (w_query, w_key, w_value, w_outgate):
        columns = weight.shape[1]
        pairs.append((weight, w_proj_v.at[:, pl.ds(at, columns)]))
        at += columns
    wait_proj = load(*pairs, whole=w_proj_v)
    wait_c = load((state_c.at[:, 0], c_v))
    wait_cell = [load((state_n, n_v)), load((state_m, m_v)), load((forget_bias, bias_v))]
    wait_out = load((w_output, w_out_v))
    ff = w_gateff.shape[0]
    ff_rows = w_ff_v.at[:, pl.ds(0, ff)]
    wait_ff = load((w_gateff, ff_rows.at[0]), (w_upff, ff_rows.at[1]), whole=ff_rows)
    wait_down = load((w_downff, w_down_v))

    def kv_copy(phase, source, target, peer):
        return pltpu.make_async_remote_copy(
            src_ref=source,
            dst_ref=target,
            send_sem=kv_send_sem.at[phase],
            recv_sem=kv_recv_sem.at[phase],
            device_id={"kv": peer},
            device_id_type=MESH,
        )

    others = pl.ds(0, kv_n - 1)
    unsent = []

    def all_sent():
        for wait in unsent:
            wait()
        unsent.clear()

    def kv_all(phase, send, recv):
        return kv_copy(phase, send.at[others], recv.at[others], kv_peer(0, 1))

    def scatter_one(phase, peer, send, recv):
        return kv_copy(phase, send.at[peer], recv.at[kv], peer)

    def scatter_all(phase, send, recv):
        for offset in around:
            scatter_one(phase, kv_peer(*offset), send, recv).start()

    def scatter_total(phase, send, recv):
        recv[kv] = send[kv]
        copies = kv_all(phase, send, recv)
        copies.wait_recv()
        unsent.append(copies.wait_send)
        total = recv[0].astype(f32)
        for peer in range(1, kv_n):
            total = total + recv[peer].astype(f32)
        return total

    def gather_start(phase, blocks):
        for offset in around:
            kv_copy(phase, blocks.at[kv], blocks.at[kv], kv_peer(*offset)).start()

    def block(group, place):
        first = place // 2
        return first * side + 2 * (place % 2) + (first + group) % 2

    def gathered(phase, blocks):
        copies = kv_all(phase, blocks, blocks)
        copies.wait_recv()
        unsent.append(copies.wait_send)
        parts = [blocks[block(group, place)] for group in range(2) for place in range(places)]
        return jnp.concatenate([part.astype(f32) for part in parts], axis=0).astype(bf16)

    def tp_copy(place, source, target, peer):
        return pltpu.make_async_remote_copy(
            src_ref=source,
            dst_ref=target,
            send_sem=tp_send_sem.at[place],
            recv_sem=tp_recv_sem.at[place],
            device_id={"tp": peer},
            device_id_type=MESH,
        )

    def tp_total(first, part, swap_send, swap_recv, quads):
        part_f32[...] = part.reshape(2, half, width)
        swap_send[...] = part_f32[1 - core].astype(bf16)
        swap = tp_copy(first, swap_send, swap_recv, partner)
        swap.start()
        swap.wait_recv()
        quads[ring] = (part_f32[core] + swap_recv[...].astype(f32)).astype(bf16)
        for offset in (2, 1, 3):
            peer = lax.rem(ring + offset, side) * 2 + core
            tp_copy(first + 1, quads.at[ring], quads.at[ring], peer).start()
        all_sent()
        three = quads.at[pl.ds(0, side - 1)]
        copies = tp_copy(first + 1, three, three, partner)
        copies.wait_recv()
        unsent.extend((swap.wait_send, copies.wait_send))
        total = quads[0].astype(f32)
        for place in range(1, side):
            total = total + quads[place].astype(f32)
        return total

    def tp_share(place, halves):
        copy = tp_copy(place, halves.at[core], halves.at[core], partner)
        copy.start()
        unsent.append(copy.wait_send)
        other = halves.at[1 - core]
        return tp_copy(place, other, other, partner).wait_recv

    wait_tok()
    wait_gains()
    tok_float = tok_v[...].astype(f32).reshape(batch, width)
    squares_one = jnp.sum(tok_float * tok_float, axis=1, keepdims=True)
    normed_one = (tok_float * gains_v[0]).astype(bf16)
    lanes = lane_ids(batch)
    gate_row = lax.broadcasted_iota(jnp.int32, (LANES, 2 * heads_all), 1)
    gate_lane = lax.broadcasted_iota(jnp.int32, (LANES, 2 * heads_all), 0)
    wanted = jnp.where(
        (gate_lane == 0) | (gate_lane == 3),
        tp,
        jnp.where((gate_lane == 1) | (gate_lane == 4), heads_all + tp, -1),
    )
    pick = jnp.where(gate_row == wanted, 1.0, 0.0).astype(bf16)
    wait_gates()
    gate_weight = dot(pick, w_gates_v[...]).astype(bf16)
    extra = dot_rows(normed_one, gate_weight)
    extra = jnp.where((lanes == 2) | (lanes == 5), squares_one, extra)
    extra_short = extra.astype(bf16).astype(f32)
    extra = jnp.where(lanes < 3, extra_short, extra - extra_short)
    qk_send[:, :, pl.ds(qk_width, LANES)] = extra.reshape(kv_n, rows, LANES).astype(bf16)
    wait_proj()
    step = 512
    for target, base, length in ((qk_send, 0, qk_width), (vo_send, qk_width, vo_width)):
        for at in range(0, length, step):
            part = dot(normed_one, w_proj_v[:, pl.ds(base + at, step)])
            target[:, :, pl.ds(at, step)] = part.reshape(kv_n, rows, step).astype(bf16)

    pl.semaphore_wait(barrier, kv_n + len(tp_peers) - 1)
    scatter_all(0, qk_send, qk_recv)
    scatter_all(1, vo_send, vo_recv)

    wait_c()
    for one in range(rows):
        c_short[one] = c_v[one].astype(bf16)
    for wait in wait_cell:
        wait()

    qk_rows = scatter_total(0, qk_send, qk_recv)
    extra = qk_rows[:, qk_width:]
    lanes = lane_ids(rows)

    def picked(lane):
        chosen = (lanes == lane) | (lanes == lane + 3)
        return jnp.sum(jnp.where(chosen, extra, 0.0), axis=1, keepdims=True)

    scale_one = lax.rsqrt(picked(2) / width_all + norm_floor)
    query = qk_rows[:, :query_size] * (scale_one * query_size ** (-0.5))
    key_vec = qk_rows[:, query_size:qk_width] * scale_one
    head_lane = lax.broadcasted_iota(jnp.int32, (1, heads_all), 1)
    bias = jnp.sum(jnp.where(head_lane == tp, bias_v[...], 0.0), axis=1, keepdims=True)
    log_input = picked(0) * scale_one
    forget_pre = picked(1) * scale_one + bias
    log_forget = -(jnp.maximum(-forget_pre, 0.0) + jnp.log1p(jnp.exp(-jnp.abs(forget_pre))))
    row_at = lax.broadcasted_iota(jnp.int32, (rows, rows), 0)
    same = row_at == lax.broadcasted_iota(jnp.int32, (rows, rows), 1)
    m_column = jnp.sum(jnp.where(same, m_v[...], 0.0), axis=1, keepdims=True)
    carried = log_forget + m_column
    m_next = jnp.maximum(carried, log_input)
    keep = jnp.exp(carried - m_next)
    admit = jnp.exp(log_input - m_next)
    n_next = keep * n_v[:, 0, :] + admit * key_vec
    denom = jnp.maximum(
        jnp.abs(jnp.sum(n_next * query, axis=1, keepdims=True)), jnp.exp(-m_next)
    )
    key_query = jnp.sum(key_vec * query, axis=1, keepdims=True)
    query_short = query.astype(bf16)
    query_rest = (query - query_short.astype(f32)).astype(bf16)
    row_ids = lax.broadcasted_iota(jnp.int32, (rows, value_size), 0)
    read = jnp.zeros((rows, value_size), f32)
    query_both = jnp.concatenate([query_short.astype(f32), query_rest.astype(f32)], axis=0).astype(bf16)
    for one in range(rows):
        product = dot_rows(query_both, c_short[one])
        read = jnp.where(row_ids == one, product[:rows] + product[rows:], read)
    kept_read = keep * read
    vo_rows = scatter_total(1, vo_send, vo_recv)
    admitted = (admit * scale_one) * vo_rows[:, :value_size]
    out_pre = vo_rows[:, value_size:] * scale_one
    numer = kept_read + admitted * key_query
    head_all[kv] = (jax.nn.sigmoid(out_pre) * numer / denom).astype(bf16)
    gather_start(2, head_all)

    new_n[:, 0, :] = n_next
    new_m[...] = jnp.sum(jnp.where(same, m_next, 0.0), axis=0, keepdims=True)
    admitted_column = admitted.T
    for one in range(rows):
        new_c[one, 0] = (
            keep[one : one + 1, :] * c_v[one]
            + admitted_column[:, one : one + 1] * key_vec[one : one + 1, :]
        )

    wait_out()
    heads = gathered(2, head_all)
    attn_part = dot(heads, w_out_v[...])
    attn_mix = tp_total(0, attn_part, attn_swap, attn_swapped, attn_quads)
    tok_half = [tok_v[block(core, place)].astype(f32) for place in range(places)]
    mid_all[core] = (jnp.concatenate(tok_half, axis=0) + attn_mix).astype(bf16)
    mid_arrived = tp_share(2, mid_all)
    wait_ff()

    lanes = lane_ids(half)
    (start_0, ff_0, wide_0), (start_1, ff_1, wide_1) = chunks

    def normed(at_half):
        mid_float = mid_all[at_half].astype(f32)
        squares = jnp.sum(mid_float * mid_float, axis=1, keepdims=True)
        return squares, (mid_float * gains_v[1]).astype(bf16)

    def ff_products(source, start, wide, send, at_half, extra):
        count = source.shape[0] // rows
        for which in range(2):
            for at in range(0, wide, step):
                columns = min(step, wide - at)
                weight = w_ff_v[which, pl.ds(start + at, columns), :]
                part = dot_rows(source, weight)
                if extra is not None and which == 0 and at + columns == wide:
                    last = jnp.where(lanes < LANES - 2, part[:, columns - LANES :], extra)
                    if columns > LANES:
                        last = jnp.concatenate([part[:, : columns - LANES], last], axis=1)
                    part = last
                part = part.reshape(count, rows, columns).astype(bf16)
                for place in range(count):
                    group = at_half if count == places else place // places
                    send[block(group, place % places), :, pl.ds(which * wide + at, columns)] = part[place]

    for turn in range(2):
        at_half = core if turn == 0 else 1 - core
        if turn == 1:
            mid_arrived()
        squares_two, normed_two = normed(at_half)
        squares_short = squares_two.astype(bf16).astype(f32)
        extra = jnp.where(lanes == LANES - 2, squares_short, squares_two - squares_short)
        ff_products(normed_two, start_0, wide_0, ff_send_0, at_half, extra)
        mine = colour == at_half
        for at_even, at_odd in zip(even, odd):
            peer = kv_peer(
                jnp.where(mine, at_even[0], at_odd[0]), jnp.where(mine, at_even[1], at_odd[1])
            )
            copy = scatter_one(3, peer, ff_send_0, ff_recv_0)
            if at_even == (0, 0):
                pl.when(jnp.logical_not(mine))(copy.start)
            else:
                copy.start()
    normed_two = jnp.concatenate([normed(0)[1], normed(1)[1]], axis=0)
    ff_products(normed_two, start_1, wide_1, ff_send_1, None, None)
    scatter_all(4, ff_send_1, ff_recv_1)

    def activated(total, columns, wide, scale):
        gate = total[:, :columns] * scale
        up = total[:, wide : wide + columns] * scale
        return (gate / (1.0 + jnp.exp(-gate)) * up).astype(bf16)

    total_0 = scatter_total(3, ff_send_0, ff_recv_0)
    rows_two = jnp.sum(total_0[:, wide_0 - 2 : wide_0], axis=1, keepdims=True)
    scale_two = lax.rsqrt(rows_two / width_all + norm_floor)
    hidden_0[kv] = activated(total_0, ff_0, wide_0, scale_two)
    gather_start(5, hidden_0)
    total_1 = scatter_total(4, ff_send_1, ff_recv_1)
    hidden_1[kv] = activated(total_1, ff_1, wide_1, scale_two)
    gather_start(6, hidden_1)

    wait_down()
    down_part = dot(gathered(5, hidden_0), w_down_v[pl.ds(start_0, ff_0), :])
    down_part = down_part + dot(gathered(6, hidden_1), w_down_v[pl.ds(start_1, ff_1), :])
    down_sum = tp_total(3, down_part, down_swap, down_swapped, down_quads)
    mixed[core] = (mid_all[core].astype(f32) + down_sum).astype(bf16)
    mixed_arrived = tp_share(5, mixed)
    mixed_arrived()
    all_sent()


def write_out(mixed, new_c, new_n, new_m, mixed_to, c_to, n_to, m_to, sem):
    kv_n = mixed_to.shape[0]
    rows, side = mixed_to.shape[1], 4
    groups = ([(new_c.at[one], c_to.at[one]) for one in range(new_c.shape[0])], [], [], [])
    groups[1].append((new_n, n_to))
    groups[2].append((new_m, m_to))
    for block in range(kv_n):
        first, second = block // side, block % side
        place = (first * 2 + second // 2) * rows
        source = mixed.at[(first + second) % 2, pl.ds(place, rows)]
        groups[3].append((source, mixed_to.at[block]))
    for at, pairs in enumerate(groups):
        for source, target in pairs:
            pltpu.make_async_copy(source, target, sem.at[at]).start()
    for at, whole in enumerate((new_c, new_n, new_m, mixed)):
        pltpu.make_async_copy(whole, whole, sem.at[at]).wait()


def solution(mesh):
    kv_n, tp_n = mesh.shape["kv"], mesh.shape["tp"]

    def per_device(*args):
        args = list(args)
        for place in (1, 7, 12):
            args[place] = args[place].reshape(1, -1)
        for place in (6, 10, 13, 14):
            args[place] = args[place].T
        tokens, w_query, w_value, state_c, w_gateff = (args[i] for i in (0, 2, 4, 8, 13))
        batch, width = tokens.shape
        rows, half = batch // kv_n, batch // 2
        args[0] = tokens.reshape(kv_n, rows, width)
        value_size, query_size = state_c.shape[2:]
        ff = w_gateff.shape[0]
        ff_pad = up_to_lanes(ff)
        second = 512
        chunks = ((second, ff - second, ff_pad - second), (0, second, second))
        proj_width = 2 * query_size + 2 * value_size
        heads_all = args[7].shape[1]
        V = pltpu.VMEM
        scratch = [
            V((kv_n, rows, width), bf16),
            V((2, 1, width), f32),
            V((width, proj_width), bf16),
            V((2 * heads_all, width), bf16),
            V((1, heads_all), f32),
            V((rows, value_size, query_size), f32),
            V((rows, 1, query_size), f32),
            V((1, rows), f32),
            V((value_size, width), bf16),
            V((2, ff_pad, width), bf16),
            V((ff, width), bf16),
            V((rows, value_size, query_size), bf16),
            V((kv_n, rows, 2 * query_size + LANES), bf16),
            V((kv_n, rows, 2 * query_size + LANES), bf16),
            V((kv_n, rows, 2 * value_size), bf16),
            V((kv_n, rows, 2 * value_size), bf16),
            V((kv_n, rows, value_size), bf16),
            V((2, half, width), f32),
            V((half, width), bf16),
            V((half, width), bf16),
            V((tp_n // 2, half, width), bf16),
            V((2, half, width), bf16),
            V((kv_n, rows, 2 * chunks[0][2]), bf16),
            V((kv_n, rows, 2 * chunks[0][2]), bf16),
            V((kv_n, rows, 2 * chunks[1][2]), bf16),
            V((kv_n, rows, 2 * chunks[1][2]), bf16),
            V((kv_n, rows, chunks[0][1]), bf16),
            V((kv_n, rows, chunks[1][1]), bf16),
            V((half, width), bf16),
            V((half, width), bf16),
            V((tp_n // 2, half, width), bf16),
            pltpu.SemaphoreType.DMA((11,)),
            pltpu.SemaphoreType.DMA((7,)),
            pltpu.SemaphoreType.DMA((7,)),
            pltpu.SemaphoreType.DMA((6,)),
            pltpu.SemaphoreType.DMA((6,)),
        ]
        anywhere = pl.BlockSpec(memory_space=pl.ANY)
        inside = pl.BlockSpec(memory_space=pltpu.VMEM)
        results = (
            ((2, half, width), bf16),
            (state_c.shape, f32),
            (args[9].shape, f32),
            (args[10].shape, f32),
        )
        outs = pl.pallas_call(
            functools.partial(layer, kv_n, tp_n, chunks),
            out_shape=tuple(V(shape, dtype) for shape, dtype in results),
            in_specs=[anywhere] * len(args),
            out_specs=(inside,) * 4,
            scratch_shapes=scratch,
            compiler_params=pltpu.CompilerParams(
                collective_id=0, has_side_effects=True, vmem_limit_bytes=58 * 1024 * 1024
            ),
        )(*args)
        results = (((kv_n, rows, width), bf16), *results[1:])
        outs = pl.pallas_call(
            write_out,
            out_shape=tuple(jax.ShapeDtypeStruct(shape, dtype) for shape, dtype in results),
            in_specs=[inside] * len(outs),
            out_specs=(anywhere,) * len(outs),
            scratch_shapes=[pltpu.SemaphoreType.DMA((len(outs),))],
            compiler_params=pltpu.CompilerParams(vmem_limit_bytes=1024 * 1024),
        )(*outs)
        return (outs[0].reshape(batch, width), outs[1], outs[2], outs[3].T)

    placed = (
        P(None, "kv"),
        P("kv"),
        P("kv", "tp"),
        P("kv", "tp"),
        P("kv", "tp"),
        P("kv", "tp"),
        P(),
        P(),
        P("kv", "tp", None, None),
        P("kv", "tp", None),
        P("kv", "tp"),
        P("tp", "kv"),
        P("kv"),
        P("kv", "tp"),
        P("kv", "tp"),
        P("tp", "kv"),
    )
    return jax.shard_map(
        per_device,
        mesh=mesh,
        in_specs=placed,
        out_specs=(P(None, "kv"), P("kv", "tp", None, None), P("kv", "tp", None), P("kv", "tp")),
        check_vma=False,
    )
```

```python
import functools

import jax
import jax.numpy as jnp
from jax import lax
from jax.experimental import pallas as pl
from jax.experimental.pallas import tpu as pltpu
from jax.sharding import PartitionSpec as P

MESH = pl.DeviceIdType.MESH
norm_floor = 1e-05
f32 = jnp.float32
bf16 = jnp.bfloat16
LANES = 128


def up_to_lanes(length):
    return (length + LANES - 1) // LANES * LANES


def dot(a, b):
    return jnp.dot(a, b, preferred_element_type=f32)


def dot_rows(a, b):
    return lax.dot_general(a, b, (((1,), (1,)), ((), ())), preferred_element_type=f32)


def lane_ids(rows):
    return lax.broadcasted_iota(jnp.int32, (rows, LANES), 1)


def layer(
    kv_n,
    tp_n,
    chunks,
    tokens,
    attn_gain,
    w_query,
    w_key,
    w_value,
    w_outgate,
    w_gates,
    forget_bias,
    state_c,
    state_n,
    state_m,
    w_output,
    mlp_gain,
    w_gateff,
    w_upff,
    w_downff,
    mixed,
    new_c,
    new_n,
    new_m,
    tok_v,
    gains_v,
    w_proj_v,
    w_gates_v,
    bias_v,
    c_v,
    n_v,
    m_v,
    w_out_v,
    w_ff_v,
    w_down_v,
    c_short,
    qk_send,
    qk_recv,
    vo_send,
    vo_recv,
    head_all,
    part_f32,
    attn_swap,
    attn_swapped,
    attn_quads,
    mid_all,
    ff_send_0,
    ff_recv_0,
    ff_send_1,
    ff_recv_1,
    hidden_0,
    hidden_1,
    down_swap,
    down_swapped,
    down_quads,
    in_sem,
    kv_send_sem,
    kv_recv_sem,
    tp_send_sem,
    tp_recv_sem,
):
    kv = lax.axis_index("kv")
    tp = lax.axis_index("tp")
    _, rows, width = tok_v.shape
    batch = kv_n * rows
    half = batch // 2
    places = kv_n // 2
    width_all = width * kv_n
    heads_all = bias_v.shape[1]
    value_size, query_size = c_v.shape[1:]
    qk_width = 2 * query_size
    vo_width = 2 * value_size

    side = 4
    near = {0: 0, 1: 1, 2: 2, 3: 1}
    kv_z, kv_y = kv // side, lax.rem(kv, side)
    ring, core = tp // 2, lax.rem(tp, 2)
    partner = ring * 2 + (1 - core)

    def far_first(offsets):
        return sorted(offsets, key=lambda offset: -near[offset[0]] - near[offset[1]])

    square = [(a, b) for a in range(side) for b in range(side)]
    spread = [(2, 2), (1, 2), (3, 2), (2, 1), (2, 3), (1, 1), (3, 3), (1, 3), (3, 1), (0, 2), (2, 0)]
    spread += [(0, 1), (0, 3), (1, 0), (3, 0)]
    first_up = sorted(range(kv_n), key=lambda at: at // side + at % side)
    around = far_first([offset for offset in square if offset != (0, 0)])
    even = far_first([offset for offset in square if sum(offset) % 2 == 0])
    odd = far_first([offset for offset in square if sum(offset) % 2 == 1])
    colour = lax.rem(kv_z + kv_y, 2)

    def kv_peer(first, second):
        return lax.rem(kv_z + first, side) * side + lax.rem(kv_y + second, side)

    barrier = pltpu.get_barrier_semaphore()

    for offset in around:
        pl.semaphore_signal(
            barrier, inc=1, device_id={"kv": kv_peer(*offset)}, device_id_type=MESH
        )
    tp_peers = [partner] + [lax.rem(ring + offset, side) * 2 + core for offset in (1, 2, 3)]
    for peer in tp_peers:
        pl.semaphore_signal(barrier, inc=1, device_id={"tp": peer}, device_id_type=MESH)

    loads = []

    def load(*pairs, whole=None):
        sem = in_sem.at[len(loads)]
        loads.append(sem)
        for source, target in pairs:
            pltpu.make_async_copy(source, target, sem).start()
        whole = pairs[0][1] if whole is None else whole
        return pltpu.make_async_copy(whole, whole, sem).wait

    wait_tok = load((tokens, tok_v))
    wait_gains = load((attn_gain, gains_v.at[0]), (mlp_gain, gains_v.at[1]), whole=gains_v)
    wait_gates = load((w_gates.at[:, pl.ds(pl.multiple_of(kv * width, width), width)], w_gates_v))
    pairs, at = [], 0
    for weight in (w_query, w_key, w_value, w_outgate):
        columns = weight.shape[1]
        pairs.append((weight, w_proj_v.at[:, pl.ds(at, columns)]))
        at += columns
    wait_proj = load(*pairs, whole=w_proj_v)
    wait_c = load((state_c.at[:, 0], c_v))
    wait_cell = [load((state_n, n_v)), load((state_m, m_v)), load((forget_bias, bias_v))]
    wait_out = load((w_output, w_out_v))
    ff = w_gateff.shape[0]
    ff_rows = w_ff_v.at[:, pl.ds(0, ff)]
    wait_ff = load((w_gateff, ff_rows.at[0]), (w_upff, ff_rows.at[1]), whole=ff_rows)
    wait_down = load((w_downff, w_down_v))

    def kv_copy(phase, source, target, peer):
        return pltpu.make_async_remote_copy(
            src_ref=source,
            dst_ref=target,
            send_sem=kv_send_sem.at[phase],
            recv_sem=kv_recv_sem.at[phase],
            device_id={"kv": peer},
            device_id_type=MESH,
        )

    others = pl.ds(0, kv_n - 1)
    unsent = []

    def all_sent():
        for wait in unsent:
            wait()
        unsent.clear()

    def kv_all(phase, send, recv):
        return kv_copy(phase, send.at[others], recv.at[others], kv_peer(0, 1))

    def scatter_one(phase, peer, send, recv):
        return kv_copy(phase, send.at[peer], recv.at[kv], peer)

    def in_order(copy_to, order):
        if order is None or isinstance(order[0], tuple):
            for offset in order or around:
                copy_to(kv_peer(*offset)).start()
        else:
            for peer in order:
                pl.when(kv != peer)(copy_to(peer).start)

    def scatter_all(phase, send, recv, order=None):
        in_order(lambda peer: scatter_one(phase, peer, send, recv), order)

    def scatter_total(phase, send, recv):
        recv[kv] = send[kv]
        copies = kv_all(phase, send, recv)
        copies.wait_recv()
        unsent.append(copies.wait_send)
        total = recv[0].astype(f32)
        for peer in range(1, kv_n):
            total = total + recv[peer].astype(f32)
        return total

    def gather_start(phase, blocks, order=None):
        in_order(lambda peer: kv_copy(phase, blocks.at[kv], blocks.at[kv], peer), order)

    def block(group, place):
        first = place // 2
        return first * side + 2 * (place % 2) + (first + group) % 2

    def gathered(phase, blocks):
        copies = kv_all(phase, blocks, blocks)
        copies.wait_recv()
        unsent.append(copies.wait_send)
        parts = [blocks[block(group, place)] for group in range(2) for place in range(places)]
        return jnp.concatenate([part.astype(f32) for part in parts], axis=0).astype(bf16)

    def tp_copy(place, source, target, peer):
        return pltpu.make_async_remote_copy(
            src_ref=source,
            dst_ref=target,
            send_sem=tp_send_sem.at[place],
            recv_sem=tp_recv_sem.at[place],
            device_id={"tp": peer},
            device_id_type=MESH,
        )

    def tp_total(first, part, swap_send, swap_recv, quads):
        part_f32[...] = part.reshape(2, half, width)
        swap_send[...] = part_f32[1 - core].astype(bf16)
        swap = tp_copy(first, swap_send, swap_recv, partner)
        swap.start()
        swap.wait_recv()
        quads[ring] = (part_f32[core] + swap_recv[...].astype(f32)).astype(bf16)
        for offset in (2, 1, 3):
            peer = lax.rem(ring + offset, side) * 2 + core
            tp_copy(first + 1, quads.at[ring], quads.at[ring], peer).start()
        all_sent()
        three = quads.at[pl.ds(0, side - 1)]
        copies = tp_copy(first + 1, three, three, partner)
        copies.wait_recv()
        unsent.extend((swap.wait_send, copies.wait_send))
        total = quads[0].astype(f32)
        for place in range(1, side):
            total = total + quads[place].astype(f32)
        return total

    def tp_share(place, halves):
        copy = tp_copy(place, halves.at[core], halves.at[core], partner)
        copy.start()
        unsent.append(copy.wait_send)
        other = halves.at[1 - core]
        return tp_copy(place, other, other, partner).wait_recv

    wait_tok()
    wait_gains()
    tok_float = tok_v[...].astype(f32).reshape(batch, width)
    squares_one = jnp.sum(tok_float * tok_float, axis=1, keepdims=True)
    normed_one = (tok_float * gains_v[0]).astype(bf16)
    lanes = lane_ids(batch)
    gate_row = lax.broadcasted_iota(jnp.int32, (LANES, 2 * heads_all), 1)
    gate_lane = lax.broadcasted_iota(jnp.int32, (LANES, 2 * heads_all), 0)
    wanted = jnp.where(
        (gate_lane == 0) | (gate_lane == 3),
        tp,
        jnp.where((gate_lane == 1) | (gate_lane == 4), heads_all + tp, -1),
    )
    pick = jnp.where(gate_row == wanted, 1.0, 0.0).astype(bf16)
    wait_gates()
    gate_weight = dot(pick, w_gates_v[...]).astype(bf16)
    extra = dot_rows(normed_one, gate_weight)
    extra = jnp.where((lanes == 2) | (lanes == 5), squares_one, extra)
    extra_short = extra.astype(bf16).astype(f32)
    extra = jnp.where(lanes < 3, extra_short, extra - extra_short)
    qk_send[:, :, pl.ds(qk_width, LANES)] = extra.reshape(kv_n, rows, LANES).astype(bf16)
    wait_proj()
    step = 512
    for target, base, length in ((qk_send, 0, qk_width), (vo_send, qk_width, vo_width)):
        for at in range(0, length, step):
            part = dot(normed_one, w_proj_v[:, pl.ds(base + at, step)])
            target[:, :, pl.ds(at, step)] = part.reshape(kv_n, rows, step).astype(bf16)

    pl.semaphore_wait(barrier, kv_n + len(tp_peers) - 1)
    scatter_all(0, qk_send, qk_recv)
    scatter_all(1, vo_send, vo_recv)

    wait_c()
    for one in range(rows):
        c_short[one] = c_v[one].astype(bf16)
    for wait in wait_cell:
        wait()

    qk_rows = scatter_total(0, qk_send, qk_recv)
    extra = qk_rows[:, qk_width:]
    lanes = lane_ids(rows)

    def picked(lane):
        chosen = (lanes == lane) | (lanes == lane + 3)
        return jnp.sum(jnp.where(chosen, extra, 0.0), axis=1, keepdims=True)

    scale_one = lax.rsqrt(picked(2) / width_all + norm_floor)
    query = qk_rows[:, :query_size] * (scale_one * query_size ** (-0.5))
    key_vec = qk_rows[:, query_size:qk_width] * scale_one
    head_lane = lax.broadcasted_iota(jnp.int32, (1, heads_all), 1)
    bias = jnp.sum(jnp.where(head_lane == tp, bias_v[...], 0.0), axis=1, keepdims=True)
    log_input = picked(0) * scale_one
    forget_pre = picked(1) * scale_one + bias
    log_forget = -(jnp.maximum(-forget_pre, 0.0) + jnp.log1p(jnp.exp(-jnp.abs(forget_pre))))
    row_at = lax.broadcasted_iota(jnp.int32, (rows, rows), 0)
    same = row_at == lax.broadcasted_iota(jnp.int32, (rows, rows), 1)
    m_column = jnp.sum(jnp.where(same, m_v[...], 0.0), axis=1, keepdims=True)
    carried = log_forget + m_column
    m_next = jnp.maximum(carried, log_input)
    keep = jnp.exp(carried - m_next)
    admit = jnp.exp(log_input - m_next)
    n_next = keep * n_v[:, 0, :] + admit * key_vec
    denom = jnp.maximum(
        jnp.abs(jnp.sum(n_next * query, axis=1, keepdims=True)), jnp.exp(-m_next)
    )
    key_query = jnp.sum(key_vec * query, axis=1, keepdims=True)
    query_short = query.astype(bf16)
    query_rest = (query - query_short.astype(f32)).astype(bf16)
    row_ids = lax.broadcasted_iota(jnp.int32, (rows, value_size), 0)
    read = jnp.zeros((rows, value_size), f32)
    query_both = jnp.concatenate([query_short.astype(f32), query_rest.astype(f32)], axis=0).astype(bf16)
    for one in range(rows):
        product = dot_rows(query_both, c_short[one])
        read = jnp.where(row_ids == one, product[:rows] + product[rows:], read)
    kept_read = keep * read
    vo_rows = scatter_total(1, vo_send, vo_recv)
    admitted = (admit * scale_one) * vo_rows[:, :value_size]
    out_pre = vo_rows[:, value_size:] * scale_one
    numer = kept_read + admitted * key_query
    head_all[kv] = (jax.nn.sigmoid(out_pre) * numer / denom).astype(bf16)
    gather_start(2, head_all)

    new_n[:, 0, :] = n_next
    new_m[...] = jnp.sum(jnp.where(same, m_next, 0.0), axis=0, keepdims=True)
    admitted_column = admitted.T
    for one in range(rows):
        new_c[one, 0] = (
            keep[one : one + 1, :] * c_v[one]
            + admitted_column[:, one : one + 1] * key_vec[one : one + 1, :]
        )

    wait_out()
    heads = gathered(2, head_all)
    attn_part = dot(heads, w_out_v[...])
    attn_mix = tp_total(0, attn_part, attn_swap, attn_swapped, attn_quads)
    tok_half = [tok_v[block(core, place)].astype(f32) for place in range(places)]
    mid_all[core] = (jnp.concatenate(tok_half, axis=0) + attn_mix).astype(bf16)
    mid_arrived = tp_share(2, mid_all)
    wait_ff()

    lanes = lane_ids(half)
    (start_0, ff_0, wide_0), (start_1, ff_1, wide_1) = chunks

    def normed(at_half):
        mid_float = mid_all[at_half].astype(f32)
        squares = jnp.sum(mid_float * mid_float, axis=1, keepdims=True)
        return squares, (mid_float * gains_v[1]).astype(bf16)

    def ff_products(source, start, wide, send, at_half, extra):
        count = source.shape[0] // rows
        for which in range(2):
            for at in range(0, wide, step):
                columns = min(step, wide - at)
                weight = w_ff_v[which, pl.ds(start + at, columns), :]
                part = dot_rows(source, weight)
                if extra is not None and which == 0 and at + columns == wide:
                    last = jnp.where(lanes < LANES - 2, part[:, columns - LANES :], extra)
                    if columns > LANES:
                        last = jnp.concatenate([part[:, : columns - LANES], last], axis=1)
                    part = last
                part = part.reshape(count, rows, columns).astype(bf16)
                for place in range(count):
                    group = at_half if count == places else place // places
                    send[block(group, place % places), :, pl.ds(which * wide + at, columns)] = part[place]

    for turn in range(2):
        at_half = core if turn == 0 else 1 - core
        if turn == 1:
            mid_arrived()
        squares_two, normed_two = normed(at_half)
        squares_short = squares_two.astype(bf16).astype(f32)
        extra = jnp.where(lanes == LANES - 2, squares_short, squares_two - squares_short)
        ff_products(normed_two, start_0, wide_0, ff_send_0, at_half, extra)
        mine = colour == at_half
        for at_even, at_odd in zip(even, odd):
            peer = kv_peer(
                jnp.where(mine, at_even[0], at_odd[0]), jnp.where(mine, at_even[1], at_odd[1])
            )
            copy = scatter_one(3, peer, ff_send_0, ff_recv_0)
            if at_even == (0, 0):
                pl.when(jnp.logical_not(mine))(copy.start)
            else:
                copy.start()
    normed_two = jnp.concatenate([normed(0)[1], normed(1)[1]], axis=0)
    ff_products(normed_two, start_1, wide_1, ff_send_1, None, None)
    scatter_all(4, ff_send_1, ff_recv_1, spread)

    def activated(total, columns, wide, scale):
        gate = total[:, :columns] * scale
        up = total[:, wide : wide + columns] * scale
        return (gate / (1.0 + jnp.exp(-gate)) * up).astype(bf16)

    total_0 = scatter_total(3, ff_send_0, ff_recv_0)
    rows_two = jnp.sum(total_0[:, wide_0 - 2 : wide_0], axis=1, keepdims=True)
    scale_two = lax.rsqrt(rows_two / width_all + norm_floor)
    hidden_0[kv] = activated(total_0, ff_0, wide_0, scale_two)
    gather_start(5, hidden_0, first_up)
    total_1 = scatter_total(4, ff_send_1, ff_recv_1)
    hidden_1[kv] = activated(total_1, ff_1, wide_1, scale_two)
    gather_start(6, hidden_1, first_up)

    wait_down()
    down_part = dot(gathered(5, hidden_0), w_down_v[pl.ds(start_0, ff_0), :])
    down_part = down_part + dot(gathered(6, hidden_1), w_down_v[pl.ds(start_1, ff_1), :])
    down_sum = tp_total(3, down_part, down_swap, down_swapped, down_quads)
    mixed[core] = (mid_all[core].astype(f32) + down_sum).astype(bf16)
    mixed_arrived = tp_share(5, mixed)
    mixed_arrived()
    all_sent()


def write_out(mixed, new_c, new_n, new_m, mixed_to, c_to, n_to, m_to, sem):
    kv_n = mixed_to.shape[0]
    rows, side = mixed_to.shape[1], 4
    groups = ([(new_c, c_to)], [], [], [])
    groups[1].append((new_n, n_to))
    groups[2].append((new_m, m_to))
    for block in range(kv_n):
        first, second = block // side, block % side
        place = (first * 2 + second // 2) * rows
        source = mixed.at[(first + second) % 2, pl.ds(place, rows)]
        groups[3].append((source, mixed_to.at[block]))
    for at, pairs in enumerate(groups):
        for source, target in pairs:
            pltpu.make_async_copy(source, target, sem.at[at]).start()
    for at, whole in enumerate((new_c, new_n, new_m, mixed)):
        pltpu.make_async_copy(whole, whole, sem.at[at]).wait()


def solution(mesh):
    kv_n, tp_n = mesh.shape["kv"], mesh.shape["tp"]

    def per_device(*args):
        args = list(args)
        for place in (1, 7, 12):
            args[place] = args[place].reshape(1, -1)
        for place in (6, 10, 13, 14):
            args[place] = args[place].T
        tokens, w_query, w_value, state_c, w_gateff = (args[i] for i in (0, 2, 4, 8, 13))
        batch, width = tokens.shape
        rows, half = batch // kv_n, batch // 2
        args[0] = tokens.reshape(kv_n, rows, width)
        value_size, query_size = state_c.shape[2:]
        ff = w_gateff.shape[0]
        ff_pad = up_to_lanes(ff)
        second = 640
        chunks = ((second, ff - second, ff_pad - second), (0, second, second))
        proj_width = 2 * query_size + 2 * value_size
        heads_all = args[7].shape[1]
        V = pltpu.VMEM
        scratch = [
            V((kv_n, rows, width), bf16),
            V((2, 1, width), f32),
            V((width, proj_width), bf16),
            V((2 * heads_all, width), bf16),
            V((1, heads_all), f32),
            V((rows, value_size, query_size), f32),
            V((rows, 1, query_size), f32),
            V((1, rows), f32),
            V((value_size, width), bf16),
            V((2, ff_pad, width), bf16),
            V((ff, width), bf16),
            V((rows, value_size, query_size), bf16),
            V((kv_n, rows, 2 * query_size + LANES), bf16),
            V((kv_n, rows, 2 * query_size + LANES), bf16),
            V((kv_n, rows, 2 * value_size), bf16),
            V((kv_n, rows, 2 * value_size), bf16),
            V((kv_n, rows, value_size), bf16),
            V((2, half, width), f32),
            V((half, width), bf16),
            V((half, width), bf16),
            V((tp_n // 2, half, width), bf16),
            V((2, half, width), bf16),
            V((kv_n, rows, 2 * chunks[0][2]), bf16),
            V((kv_n, rows, 2 * chunks[0][2]), bf16),
            V((kv_n, rows, 2 * chunks[1][2]), bf16),
            V((kv_n, rows, 2 * chunks[1][2]), bf16),
            V((kv_n, rows, chunks[0][1]), bf16),
            V((kv_n, rows, chunks[1][1]), bf16),
            V((half, width), bf16),
            V((half, width), bf16),
            V((tp_n // 2, half, width), bf16),
            pltpu.SemaphoreType.DMA((11,)),
            pltpu.SemaphoreType.DMA((7,)),
            pltpu.SemaphoreType.DMA((7,)),
            pltpu.SemaphoreType.DMA((6,)),
            pltpu.SemaphoreType.DMA((6,)),
        ]
        anywhere = pl.BlockSpec(memory_space=pl.ANY)
        inside = pl.BlockSpec(memory_space=pltpu.VMEM)
        results = (
            ((2, half, width), bf16),
            (state_c.shape, f32),
            (args[9].shape, f32),
            (args[10].shape, f32),
        )
        outs = pl.pallas_call(
            functools.partial(layer, kv_n, tp_n, chunks),
            out_shape=tuple(V(shape, dtype) for shape, dtype in results),
            in_specs=[anywhere] * len(args),
            out_specs=(inside,) * 4,
            scratch_shapes=scratch,
            compiler_params=pltpu.CompilerParams(
                collective_id=0, has_side_effects=True, vmem_limit_bytes=58 * 1024 * 1024
            ),
        )(*args)
        results = (((kv_n, rows, width), bf16), *results[1:])
        outs = pl.pallas_call(
            write_out,
            out_shape=tuple(jax.ShapeDtypeStruct(shape, dtype) for shape, dtype in results),
            in_specs=[inside] * len(outs),
            out_specs=(anywhere,) * len(outs),
            scratch_shapes=[pltpu.SemaphoreType.DMA((len(outs),))],
            compiler_params=pltpu.CompilerParams(vmem_limit_bytes=1024 * 1024),
        )(*outs)
        return (outs[0].reshape(batch, width), outs[1], outs[2], outs[3].T)

    placed = (
        P(None, "kv"),
        P("kv"),
        P("kv", "tp"),
        P("kv", "tp"),
        P("kv", "tp"),
        P("kv", "tp"),
        P(),
        P(),
        P("kv", "tp", None, None),
        P("kv", "tp", None),
        P("kv", "tp"),
        P("tp", "kv"),
        P("kv"),
        P("kv", "tp"),
        P("kv", "tp"),
        P("tp", "kv"),
    )
    return jax.shard_map(
        per_device,
        mesh=mesh,
        in_specs=placed,
        out_specs=(P(None, "kv"), P("kv", "tp", None, None), P("kv", "tp", None), P("kv", "tp")),
        check_vma=False,
    )
```

```python
import functools

import jax
import jax.numpy as jnp
from jax import lax
from jax.experimental import pallas as pl
from jax.experimental.pallas import tpu as pltpu
from jax.sharding import PartitionSpec as P

MESH = pl.DeviceIdType.MESH
norm_floor = 1e-05
f32 = jnp.float32
bf16 = jnp.bfloat16
LANES = 128


def up_to_lanes(length):
    return (length + LANES - 1) // LANES * LANES


def dot(a, b):
    return jnp.dot(a, b, preferred_element_type=f32)


def dot_rows(a, b):
    return lax.dot_general(a, b, (((1,), (1,)), ((), ())), preferred_element_type=f32)


def lane_ids(rows):
    return lax.broadcasted_iota(jnp.int32, (rows, LANES), 1)


def layer(
    kv_n,
    tp_n,
    chunks,
    tokens,
    attn_gain,
    w_query,
    w_key,
    w_value,
    w_outgate,
    w_gates,
    forget_bias,
    state_c,
    state_n,
    state_m,
    w_output,
    mlp_gain,
    w_gateff,
    w_upff,
    w_downff,
    mixed,
    new_c,
    new_n,
    new_m,
    tok_v,
    gains_v,
    w_proj_v,
    w_gates_v,
    bias_v,
    c_v,
    n_v,
    m_v,
    w_out_v,
    w_ff_v,
    w_down_v,
    c_short,
    qk_send,
    qk_recv,
    vo_send,
    vo_recv,
    head_all,
    part_f32,
    attn_swap,
    attn_swapped,
    attn_quads,
    mid_all,
    ff_send_0,
    ff_recv_0,
    ff_send_1,
    ff_recv_1,
    hidden_0,
    hidden_1,
    down_swap,
    down_swapped,
    down_quads,
    in_sem,
    kv_send_sem,
    kv_recv_sem,
    tp_send_sem,
    tp_recv_sem,
):
    kv = lax.axis_index("kv")
    tp = lax.axis_index("tp")
    _, rows, width = tok_v.shape
    batch = kv_n * rows
    half = batch // 2
    places = kv_n // 2
    width_all = width * kv_n
    heads_all = bias_v.shape[1]
    value_size, query_size = c_v.shape[1:]
    qk_width = 2 * query_size
    vo_width = 2 * value_size

    side = 4
    near = {0: 0, 1: 1, 2: 2, 3: 1}
    kv_z, kv_y = kv // side, lax.rem(kv, side)
    ring, core = tp // 2, lax.rem(tp, 2)
    partner = ring * 2 + (1 - core)

    def far_first(offsets):
        return sorted(offsets, key=lambda offset: -near[offset[0]] - near[offset[1]])

    square = [(a, b) for a in range(side) for b in range(side)]
    spread = [(2, 2), (1, 2), (3, 2), (2, 1), (2, 3), (1, 1), (3, 3), (1, 3), (3, 1), (0, 2), (2, 0)]
    spread += [(0, 1), (0, 3), (1, 0), (3, 0)]
    first_up = sorted(range(kv_n), key=lambda at: at // side + at % side)
    first_served = [0, 1, 4, 5, 3, 12, 15, 2, 8, 10, 6, 9, 7, 13, 11, 14]
    around = far_first([offset for offset in square if offset != (0, 0)])
    even = far_first([offset for offset in square if sum(offset) % 2 == 0])
    odd = far_first([offset for offset in square if sum(offset) % 2 == 1])
    colour = lax.rem(kv_z + kv_y, 2)

    def kv_peer(first, second):
        return lax.rem(kv_z + first, side) * side + lax.rem(kv_y + second, side)

    barrier = pltpu.get_barrier_semaphore()

    for offset in around:
        pl.semaphore_signal(
            barrier, inc=1, device_id={"kv": kv_peer(*offset)}, device_id_type=MESH
        )
    tp_peers = [partner] + [lax.rem(ring + offset, side) * 2 + core for offset in (1, 2, 3)]
    for peer in tp_peers:
        pl.semaphore_signal(barrier, inc=1, device_id={"tp": peer}, device_id_type=MESH)

    loads = []

    def load(*pairs, whole=None):
        sem = in_sem.at[len(loads)]
        loads.append(sem)
        for source, target in pairs:
            pltpu.make_async_copy(source, target, sem).start()
        whole = pairs[0][1] if whole is None else whole
        return pltpu.make_async_copy(whole, whole, sem).wait

    wait_tok = load((tokens, tok_v))
    wait_gains = load((attn_gain, gains_v.at[0]), (mlp_gain, gains_v.at[1]), whole=gains_v)
    wait_gates = load((w_gates.at[:, pl.ds(pl.multiple_of(kv * width, width), width)], w_gates_v))
    pairs, at = [], 0
    for weight in (w_query, w_key, w_value, w_outgate):
        columns = weight.shape[1]
        pairs.append((weight, w_proj_v.at[:, pl.ds(at, columns)]))
        at += columns
    wait_proj = load(*pairs, whole=w_proj_v)
    wait_c = load((state_c.at[:, 0], c_v))
    wait_cell = [load((state_n, n_v)), load((state_m, m_v)), load((forget_bias, bias_v))]
    wait_out = load((w_output, w_out_v))
    ff = w_gateff.shape[0]
    ff_rows = w_ff_v.at[:, pl.ds(0, ff)]
    wait_ff = load((w_gateff, ff_rows.at[0]), (w_upff, ff_rows.at[1]), whole=ff_rows)
    wait_down = load((w_downff, w_down_v))

    def kv_copy(phase, source, target, peer):
        return pltpu.make_async_remote_copy(
            src_ref=source,
            dst_ref=target,
            send_sem=kv_send_sem.at[phase],
            recv_sem=kv_recv_sem.at[phase],
            device_id={"kv": peer},
            device_id_type=MESH,
        )

    others = pl.ds(0, kv_n - 1)
    unsent = []

    def all_sent():
        for wait in unsent:
            wait()
        unsent.clear()

    def kv_all(phase, send, recv):
        return kv_copy(phase, send.at[others], recv.at[others], kv_peer(0, 1))

    def scatter_one(phase, peer, send, recv):
        return kv_copy(phase, send.at[peer], recv.at[kv], peer)

    def in_order(copy_to, order):
        if order is None or isinstance(order[0], tuple):
            for offset in order or around:
                copy_to(kv_peer(*offset)).start()
        else:
            for peer in order:
                pl.when(kv != peer)(copy_to(peer).start)

    def scatter_all(phase, send, recv, order=None):
        in_order(lambda peer: scatter_one(phase, peer, send, recv), order)

    def scatter_total(phase, send, recv):
        recv[kv] = send[kv]
        copies = kv_all(phase, send, recv)
        copies.wait_recv()
        unsent.append(copies.wait_send)
        total = recv[0].astype(f32)
        for peer in range(1, kv_n):
            total = total + recv[peer].astype(f32)
        return total

    def gather_start(phase, blocks, order=None):
        in_order(lambda peer: kv_copy(phase, blocks.at[kv], blocks.at[kv], peer), order)

    def block(group, place):
        first = place // 2
        return first * side + 2 * (place % 2) + (first + group) % 2

    def gathered(phase, blocks):
        copies = kv_all(phase, blocks, blocks)
        copies.wait_recv()
        unsent.append(copies.wait_send)
        parts = [blocks[block(group, place)] for group in range(2) for place in range(places)]
        return jnp.concatenate([part.astype(f32) for part in parts], axis=0).astype(bf16)

    def tp_copy(place, source, target, peer):
        return pltpu.make_async_remote_copy(
            src_ref=source,
            dst_ref=target,
            send_sem=tp_send_sem.at[place],
            recv_sem=tp_recv_sem.at[place],
            device_id={"tp": peer},
            device_id_type=MESH,
        )

    def tp_total(first, part, swap_send, swap_recv, quads):
        part_f32[...] = part.reshape(2, half, width)
        swap_send[...] = part_f32[1 - core].astype(bf16)
        swap = tp_copy(first, swap_send, swap_recv, partner)
        swap.start()
        swap.wait_recv()
        quads[ring] = (part_f32[core] + swap_recv[...].astype(f32)).astype(bf16)
        for offset in (2, 1, 3):
            peer = lax.rem(ring + offset, side) * 2 + core
            tp_copy(first + 1, quads.at[ring], quads.at[ring], peer).start()
        all_sent()
        three = quads.at[pl.ds(0, side - 1)]
        copies = tp_copy(first + 1, three, three, partner)
        copies.wait_recv()
        unsent.extend((swap.wait_send, copies.wait_send))
        total = quads[0].astype(f32)
        for place in range(1, side):
            total = total + quads[place].astype(f32)
        return total

    def tp_share(place, halves):
        copy = tp_copy(place, halves.at[core], halves.at[core], partner)
        copy.start()
        unsent.append(copy.wait_send)
        other = halves.at[1 - core]
        return tp_copy(place, other, other, partner).wait_recv

    wait_tok()
    wait_gains()
    tok_float = tok_v[...].astype(f32).reshape(batch, width)
    squares_one = jnp.sum(tok_float * tok_float, axis=1, keepdims=True)
    normed_one = (tok_float * gains_v[0]).astype(bf16)
    lanes = lane_ids(batch)
    gate_row = lax.broadcasted_iota(jnp.int32, (LANES, 2 * heads_all), 1)
    gate_lane = lax.broadcasted_iota(jnp.int32, (LANES, 2 * heads_all), 0)
    wanted = jnp.where(
        (gate_lane == 0) | (gate_lane == 3),
        tp,
        jnp.where((gate_lane == 1) | (gate_lane == 4), heads_all + tp, -1),
    )
    pick = jnp.where(gate_row == wanted, 1.0, 0.0).astype(bf16)
    wait_gates()
    gate_weight = dot(pick, w_gates_v[...]).astype(bf16)
    extra = dot_rows(normed_one, gate_weight)
    extra = jnp.where((lanes == 2) | (lanes == 5), squares_one, extra)
    extra_short = extra.astype(bf16).astype(f32)
    extra = jnp.where(lanes < 3, extra_short, extra - extra_short)
    qk_send[:, :, pl.ds(qk_width, LANES)] = extra.reshape(kv_n, rows, LANES).astype(bf16)
    wait_proj()
    step = 512
    for target, base, length in ((qk_send, 0, qk_width), (vo_send, qk_width, vo_width)):
        for at in range(0, length, step):
            part = dot(normed_one, w_proj_v[:, pl.ds(base + at, step)])
            target[:, :, pl.ds(at, step)] = part.reshape(kv_n, rows, step).astype(bf16)

    pl.semaphore_wait(barrier, kv_n + len(tp_peers) - 1)
    scatter_all(0, qk_send, qk_recv)
    scatter_all(1, vo_send, vo_recv)

    wait_c()
    for one in range(rows):
        c_short[one] = c_v[one].astype(bf16)
    for wait in wait_cell:
        wait()

    qk_rows = scatter_total(0, qk_send, qk_recv)
    extra = qk_rows[:, qk_width:]
    lanes = lane_ids(rows)

    def picked(lane):
        chosen = (lanes == lane) | (lanes == lane + 3)
        return jnp.sum(jnp.where(chosen, extra, 0.0), axis=1, keepdims=True)

    scale_one = lax.rsqrt(picked(2) / width_all + norm_floor)
    query = qk_rows[:, :query_size] * (scale_one * query_size ** (-0.5))
    key_vec = qk_rows[:, query_size:qk_width] * scale_one
    head_lane = lax.broadcasted_iota(jnp.int32, (1, heads_all), 1)
    bias = jnp.sum(jnp.where(head_lane == tp, bias_v[...], 0.0), axis=1, keepdims=True)
    log_input = picked(0) * scale_one
    forget_pre = picked(1) * scale_one + bias
    log_forget = -(jnp.maximum(-forget_pre, 0.0) + jnp.log1p(jnp.exp(-jnp.abs(forget_pre))))
    row_at = lax.broadcasted_iota(jnp.int32, (rows, rows), 0)
    same = row_at == lax.broadcasted_iota(jnp.int32, (rows, rows), 1)
    m_column = jnp.sum(jnp.where(same, m_v[...], 0.0), axis=1, keepdims=True)
    carried = log_forget + m_column
    m_next = jnp.maximum(carried, log_input)
    keep = jnp.exp(carried - m_next)
    admit = jnp.exp(log_input - m_next)
    n_next = keep * n_v[:, 0, :] + admit * key_vec
    denom = jnp.maximum(
        jnp.abs(jnp.sum(n_next * query, axis=1, keepdims=True)), jnp.exp(-m_next)
    )
    key_query = jnp.sum(key_vec * query, axis=1, keepdims=True)
    query_short = query.astype(bf16)
    query_rest = (query - query_short.astype(f32)).astype(bf16)
    row_ids = lax.broadcasted_iota(jnp.int32, (rows, value_size), 0)
    read = jnp.zeros((rows, value_size), f32)
    query_both = jnp.concatenate([query_short.astype(f32), query_rest.astype(f32)], axis=0).astype(bf16)
    for one in range(rows):
        product = dot_rows(query_both, c_short[one])
        read = jnp.where(row_ids == one, product[:rows] + product[rows:], read)
    kept_read = keep * read
    vo_rows = scatter_total(1, vo_send, vo_recv)
    admitted = (admit * scale_one) * vo_rows[:, :value_size]
    out_pre = vo_rows[:, value_size:] * scale_one
    numer = kept_read + admitted * key_query
    head_all[kv] = (jax.nn.sigmoid(out_pre) * numer / denom).astype(bf16)
    gather_start(2, head_all, spread)

    new_n[:, 0, :] = n_next
    new_m[...] = jnp.sum(jnp.where(same, m_next, 0.0), axis=0, keepdims=True)
    admitted_column = admitted.T
    for one in range(rows):
        new_c[one, 0] = (
            keep[one : one + 1, :] * c_v[one]
            + admitted_column[:, one : one + 1] * key_vec[one : one + 1, :]
        )

    wait_out()
    heads = gathered(2, head_all)
    attn_part = dot(heads, w_out_v[...])
    attn_mix = tp_total(0, attn_part, attn_swap, attn_swapped, attn_quads)
    tok_half = [tok_v[block(core, place)].astype(f32) for place in range(places)]
    mid_all[core] = (jnp.concatenate(tok_half, axis=0) + attn_mix).astype(bf16)
    mid_arrived = tp_share(2, mid_all)
    wait_ff()

    lanes = lane_ids(half)
    (start_0, ff_0, wide_0), (start_1, ff_1, wide_1) = chunks

    def normed(at_half):
        mid_float = mid_all[at_half].astype(f32)
        squares = jnp.sum(mid_float * mid_float, axis=1, keepdims=True)
        return squares, (mid_float * gains_v[1]).astype(bf16)

    def ff_products(source, start, wide, send, at_half, extra):
        count = source.shape[0] // rows
        for which in range(2):
            for at in range(0, wide, step):
                columns = min(step, wide - at)
                weight = w_ff_v[which, pl.ds(start + at, columns), :]
                part = dot_rows(source, weight)
                if extra is not None and which == 0 and at + columns == wide:
                    last = jnp.where(lanes < LANES - 2, part[:, columns - LANES :], extra)
                    if columns > LANES:
                        last = jnp.concatenate([part[:, : columns - LANES], last], axis=1)
                    part = last
                part = part.reshape(count, rows, columns).astype(bf16)
                for place in range(count):
                    group = at_half if count == places else place // places
                    send[block(group, place % places), :, pl.ds(which * wide + at, columns)] = part[place]

    for turn in range(2):
        at_half = core if turn == 0 else 1 - core
        if turn == 1:
            mid_arrived()
        squares_two, normed_two = normed(at_half)
        squares_short = squares_two.astype(bf16).astype(f32)
        extra = jnp.where(lanes == LANES - 2, squares_short, squares_two - squares_short)
        ff_products(normed_two, start_0, wide_0, ff_send_0, at_half, extra)
        mine = colour == at_half
        for at_even, at_odd in zip(even, odd):
            peer = kv_peer(
                jnp.where(mine, at_even[0], at_odd[0]), jnp.where(mine, at_even[1], at_odd[1])
            )
            copy = scatter_one(3, peer, ff_send_0, ff_recv_0)
            if at_even == (0, 0):
                pl.when(jnp.logical_not(mine))(copy.start)
            else:
                copy.start()
    normed_two = jnp.concatenate([normed(0)[1], normed(1)[1]], axis=0)
    ff_products(normed_two, start_1, wide_1, ff_send_1, None, None)
    scatter_all(4, ff_send_1, ff_recv_1, spread)

    def activated(total, columns, wide, scale):
        gate = total[:, :columns] * scale
        up = total[:, wide : wide + columns] * scale
        return (gate / (1.0 + jnp.exp(-gate)) * up).astype(bf16)

    total_0 = scatter_total(3, ff_send_0, ff_recv_0)
    rows_two = jnp.sum(total_0[:, wide_0 - 2 : wide_0], axis=1, keepdims=True)
    scale_two = lax.rsqrt(rows_two / width_all + norm_floor)
    hidden_0[kv] = activated(total_0, ff_0, wide_0, scale_two)
    gather_start(5, hidden_0, first_up)
    total_1 = scatter_total(4, ff_send_1, ff_recv_1)
    hidden_1[kv] = activated(total_1, ff_1, wide_1, scale_two)
    gather_start(6, hidden_1, first_served)

    wait_down()
    down_part = dot(gathered(5, hidden_0), w_down_v[pl.ds(start_0, ff_0), :])
    down_part = down_part + dot(gathered(6, hidden_1), w_down_v[pl.ds(start_1, ff_1), :])
    down_sum = tp_total(3, down_part, down_swap, down_swapped, down_quads)
    mixed[core] = (mid_all[core].astype(f32) + down_sum).astype(bf16)
    mixed_arrived = tp_share(5, mixed)
    mixed_arrived()
    all_sent()


def write_out(mixed, new_c, new_n, new_m, mixed_to, c_to, n_to, m_to, sem):
    kv_n = mixed_to.shape[0]
    rows, side = mixed_to.shape[1], 4
    groups = ([(new_c, c_to)], [], [], [])
    groups[1].append((new_n, n_to))
    groups[2].append((new_m, m_to))
    for block in range(kv_n):
        first, second = block // side, block % side
        place = (first * 2 + second // 2) * rows
        source = mixed.at[(first + second) % 2, pl.ds(place, rows)]
        groups[3].append((source, mixed_to.at[block]))
    for at, pairs in enumerate(groups):
        for source, target in pairs:
            pltpu.make_async_copy(source, target, sem.at[at]).start()
    for at, whole in enumerate((new_c, new_n, new_m, mixed)):
        pltpu.make_async_copy(whole, whole, sem.at[at]).wait()


def solution(mesh):
    kv_n, tp_n = mesh.shape["kv"], mesh.shape["tp"]

    def per_device(*args):
        args = list(args)
        for place in (1, 7, 12):
            args[place] = args[place].reshape(1, -1)
        for place in (6, 10, 13, 14):
            args[place] = args[place].T
        tokens, w_query, w_value, state_c, w_gateff = (args[i] for i in (0, 2, 4, 8, 13))
        batch, width = tokens.shape
        rows, half = batch // kv_n, batch // 2
        args[0] = tokens.reshape(kv_n, rows, width)
        value_size, query_size = state_c.shape[2:]
        ff = w_gateff.shape[0]
        ff_pad = up_to_lanes(ff)
        second = 640
        chunks = ((second, ff - second, ff_pad - second), (0, second, second))
        proj_width = 2 * query_size + 2 * value_size
        heads_all = args[7].shape[1]
        V = pltpu.VMEM
        scratch = [
            V((kv_n, rows, width), bf16),
            V((2, 1, width), f32),
            V((width, proj_width), bf16),
            V((2 * heads_all, width), bf16),
            V((1, heads_all), f32),
            V((rows, value_size, query_size), f32),
            V((rows, 1, query_size), f32),
            V((1, rows), f32),
            V((value_size, width), bf16),
            V((2, ff_pad, width), bf16),
            V((ff, width), bf16),
            V((rows, value_size, query_size), bf16),
            V((kv_n, rows, 2 * query_size + LANES), bf16),
            V((kv_n, rows, 2 * query_size + LANES), bf16),
            V((kv_n, rows, 2 * value_size), bf16),
            V((kv_n, rows, 2 * value_size), bf16),
            V((kv_n, rows, value_size), bf16),
            V((2, half, width), f32),
            V((half, width), bf16),
            V((half, width), bf16),
            V((tp_n // 2, half, width), bf16),
            V((2, half, width), bf16),
            V((kv_n, rows, 2 * chunks[0][2]), bf16),
            V((kv_n, rows, 2 * chunks[0][2]), bf16),
            V((kv_n, rows, 2 * chunks[1][2]), bf16),
            V((kv_n, rows, 2 * chunks[1][2]), bf16),
            V((kv_n, rows, chunks[0][1]), bf16),
            V((kv_n, rows, chunks[1][1]), bf16),
            V((half, width), bf16),
            V((half, width), bf16),
            V((tp_n // 2, half, width), bf16),
            pltpu.SemaphoreType.DMA((11,)),
            pltpu.SemaphoreType.DMA((7,)),
            pltpu.SemaphoreType.DMA((7,)),
            pltpu.SemaphoreType.DMA((6,)),
            pltpu.SemaphoreType.DMA((6,)),
        ]
        anywhere = pl.BlockSpec(memory_space=pl.ANY)
        inside = pl.BlockSpec(memory_space=pltpu.VMEM)
        results = (
            ((2, half, width), bf16),
            (state_c.shape, f32),
            (args[9].shape, f32),
            (args[10].shape, f32),
        )
        outs = pl.pallas_call(
            functools.partial(layer, kv_n, tp_n, chunks),
            out_shape=tuple(V(shape, dtype) for shape, dtype in results),
            in_specs=[anywhere] * len(args),
            out_specs=(inside,) * 4,
            scratch_shapes=scratch,
            compiler_params=pltpu.CompilerParams(
                collective_id=0, has_side_effects=True, vmem_limit_bytes=58 * 1024 * 1024
            ),
        )(*args)
        results = (((kv_n, rows, width), bf16), *results[1:])
        outs = pl.pallas_call(
            write_out,
            out_shape=tuple(jax.ShapeDtypeStruct(shape, dtype) for shape, dtype in results),
            in_specs=[inside] * len(outs),
            out_specs=(anywhere,) * len(outs),
            scratch_shapes=[pltpu.SemaphoreType.DMA((len(outs),))],
            compiler_params=pltpu.CompilerParams(vmem_limit_bytes=1024 * 1024),
        )(*outs)
        return (outs[0].reshape(batch, width), outs[1], outs[2], outs[3].T)

    placed = (
        P(None, "kv"),
        P("kv"),
        P("kv", "tp"),
        P("kv", "tp"),
        P("kv", "tp"),
        P("kv", "tp"),
        P(),
        P(),
        P("kv", "tp", None, None),
        P("kv", "tp", None),
        P("kv", "tp"),
        P("tp", "kv"),
        P("kv"),
        P("kv", "tp"),
        P("kv", "tp"),
        P("tp", "kv"),
    )
    return jax.shard_map(
        per_device,
        mesh=mesh,
        in_specs=placed,
        out_specs=(P(None, "kv"), P("kv", "tp", None, None), P("kv", "tp", None), P("kv", "tp")),
        check_vma=False,
    )
```
